512 devices in a mesh: sp: 32 (over z, x), tp: 16 (over y, core).
Axes of the slice: x: 4, y: 8, z: 8, core: 2. Of those that a mesh axis runs over, the one named last changes fastest.
Arguments:
- mixer_out: bfloat16 [4096, 2048], P('sp', 'tp'), may hold values from -12 to 12
- layer_grad: bfloat16 [4096, 2048], P('sp', 'tp'), may hold values from -6 to 6
- row_scale: float32 [4096], P('sp'), may hold values from 0.3 to 3
- norm_gain: bfloat16 [2048], replicated, may hold values from 0.099609375 to 1.8984375
- routes: int32 [4096, 2], P('sp'), may hold values from 0 to 31, all different within a row; in each aligned block of 128 rows (0 to 127, 128 to 255, ...) at most 16 rows name the same one
- route_weight: float32 [4096, 2], P('sp'), may hold values from 0.05 to 0.35
- expert_gate: bfloat16 [32, 3584, 2048], P('sp', 'tp'), may hold values from -0.125 to 0.125
- expert_up: bfloat16 [32, 3584, 2048], P('sp', 'tp'), may hold values from -0.125 to 0.125
- expert_down: bfloat16 [32, 3584, 2048], P('sp', 'tp'), may hold values from -0.09375 to 0.09375
- query_rows: bfloat16 [4096, 1024], P('sp', 'tp'), may hold values from -6 to 6
- key_rows: bfloat16 [4096, 1024], P('sp', 'tp'), may hold values from -6 to 6
- value_rows: bfloat16 [4096, 1024], P('sp', 'tp'), may hold values from -6 to 6
- retained: bfloat16 [4096, 1024], P('sp', 'tp'), may hold values from -6 to 6
- log_decay: float32 [16, 4096], P('tp', 'sp'), may hold values from -0.8 to 0
- entry_state: float32 [32, 16, 64, 64], P('sp', 'tp'), may hold values from -12 to 12
- out_proj: bfloat16 [1024, 2048], P('tp'), may hold values from -0.1875 to 0.1875
Outputs:
- grad_up: bfloat16 [32, 3584, 2048], P('sp', 'tp')
- grad_down: bfloat16 [32, 3584, 2048], P('sp', 'tp')
- grad_proj: float32 [2048, 1024], P('sp', 'tp')
- grad_query: bfloat16 [4096, 1024], P('sp', 'tp')
- grad_key: bfloat16 [4096, 1024], P('sp', 'tp')
- grad_value: bfloat16 [4096, 1024], P('sp', 'tp')
- stream_grad: bfloat16 [4096, 2048], P('sp', 'tp')
The draws below stay inside these ranges and needn't reach their ends.
Inputs may be any that keep to these rules, and one draw needn't show every extreme that they name: `routes`: each row names 2 different experts. Among the entries of one block of 128 consecutive rows no expert appears more than 16 times, and in every draw some block names some expert exactly 16 times.
All inputs are finite; a program needn't handle non-finite values.
Results may differ from the reference program's by a relative error of at most 0.025.
Values may be sent and summed in bfloat16 or wider, within the bound.
A program may use at most 64 MiB of HBM per device.

```python
import math
import jax
import jax.numpy as jnp
import numpy as np
from jax import lax

D = 2048
FF = 3584
HEADS = 16
HEAD_DIM = 64
TOP = 2
TOK_DEV = 128
TOKENS = 4096
EXPERTS = 32
CAP = 16
RET_W = 1024
N_SP = 32
N_TP = 16


def draw_log_decay(key, part):
    base = jax.random.fold_in(key, 7)
    pick_key, fast_key, slow_key, block_key, rough_key, spot_key, depth_key = jax.random.split(base, 7)
    share = 0.5
    fast = jax.random.uniform(pick_key, (HEADS, 1)) < share
    fast_rate = jnp.exp(jax.random.uniform(fast_key, (HEADS, 1), minval=jnp.log(1.0 / 50.0), maxval=jnp.log(1.0 / 20.0)))
    slow_rate = jnp.exp(jax.random.uniform(slow_key, (HEADS, 1), minval=jnp.log(0.15), maxval=jnp.log(0.5))) / TOKENS
    decay_rate = jnp.where(fast, fast_rate, slow_rate)
    decay_factor = jnp.exp(jax.random.uniform(block_key, (HEADS, TOKENS // TOK_DEV), minval=jnp.log(0.5), maxval=jnp.log(2.0)))
    decay_factor = jnp.repeat(decay_factor, TOK_DEV, axis=1)
    coarse_estimate = jax.random.uniform(rough_key, (HEADS, TOKENS), minval=0.5, maxval=1.5)
    spots = jax.random.randint(spot_key, (HEADS, 2), 0, TOKENS)
    layer_depth_level = jnp.log(jax.random.uniform(depth_key, (HEADS, 2), minval=0.55, maxval=0.8))
    position_index = jnp.arange(TOKENS)[None, :, None] == spots[:, None, :]
    retention_spurt = jnp.sum(jnp.where(position_index, layer_depth_level[:, None, :], 0.0), axis=2)
    return (retention_spurt - decay_rate * decay_factor * coarse_estimate).astype(jnp.float32)


def draw_mixer_out(key, part):
    base = jax.random.fold_in(key, 13)
    value_key = jax.random.fold_in(base, 0)
    ascending_decay = jnp.exp(jnp.linspace(0.0, jnp.log(4.0), D))[None, :]
    value = jax.random.normal(value_key, (TOKENS, D)) * ascending_decay
    return jnp.clip(value, -12.0, 12.0).astype(jnp.bfloat16)


def strengthened(result, own_key, source, target, parts, factor):
    owner, partner = [(jnp.arange(result.shape[dim]) // (result.shape[dim] // parts)).reshape([-1 if axis == dim else 1 for axis in range(result.ndim)]) for dim in (source, target)]
    chosen = jax.random.permutation(own_key, parts)[partner]
    strong = (owner == chosen) | (owner == (partner + parts // 2) % parts)
    return jnp.where(strong, factor * result, result)


def level_of(rng, dims, cuts, smallest, high):
    factor_of, own = 1.0, jax.random.fold_in(rng, 6)
    for axis_at, blocks in cuts:
        draws = jnp.exp(jax.random.uniform(jax.random.fold_in(own, axis_at), (blocks,), jnp.float32, smallest / len(cuts), high / len(cuts)))
        factor_of = factor_of * jnp.repeat(draws, dims[axis_at] // blocks).reshape([-1 if axis == axis_at else 1 for axis in range(len(dims))])
    return factor_of


def routed_block(own_key, own, number, rows, amount, top, most, lean):
    ranking = jax.random.permutation(own_key, amount)
    packed, usual = load_shares(amount, rows * top, most, lean, True), load_shares(amount, rows * top, most, lean, False)
    places = jnp.arange(amount)

    def named(tallies, offset_by):
        used = int((tallies > 0).sum())
        fixed = max(1, used // 4)
        moved = fixed + (places - fixed + offset_by * (used - fixed)) % max(1, amount - fixed)
        return jnp.zeros((amount,), jnp.int32).at[ranking[jnp.where(places < fixed, places, moved)]].set(jnp.asarray(tallies, jnp.int32))

    tallies = jnp.where(number % 4 == 0, named(packed, number // 4), named(usual, number - number // 4 - 1))
    mixed = jax.random.permutation(jax.random.fold_in(own, 3), amount)
    donor, sink = mixed[0:amount // 2 * 2:2], mixed[1:amount // 2 * 2:2]
    room = jnp.minimum(tallies[donor] - 1, most - tallies[sink]) // 2
    room = jnp.where((donor == ranking[0]) | (sink == ranking[0]) | (tallies[sink] == 0), 0, jnp.maximum(room, 0))
    moved = jax.random.randint(jax.random.fold_in(own, 4), (amount // 2,), 0, 1 << 20) % (room + 1)
    tallies = tallies.at[donor].add(-moved).at[sink].add(moved)
    items = jnp.searchsorted(jnp.cumsum(tallies), jnp.arange(rows * top), side="right").astype(jnp.int32)
    table = items.reshape(top, rows).T
    table = table[jax.random.permutation(jax.random.fold_in(own, 1), rows)]
    offset_by = jax.random.randint(jax.random.fold_in(own, 2), (rows, 1), 0, top)
    return jnp.take_along_axis(table, (jnp.arange(top)[None, :] + offset_by) % top, axis=1)


def load_shares(number_of, total, limit, skew, full):
    loads = [(1 << 20) // math.isqrt(rank ** skew) + 1 for rank in range(1, number_of + 1)]
    largest = limit if full else min(limit, max(-(-total // number_of), total * loads[0] // sum(loads)))
    least = 1 if total - largest >= number_of - 1 else 0
    counts, surplus = [largest] + [least] * (number_of - 1), total - largest - least * (number_of - 1)
    while surplus > 0:
        free = [i for i in range(1, number_of) if counts[i] < largest] or [i for i in range(1, number_of) if counts[i] < limit]
        pool, left = sum([loads[i] for i in free]), surplus
        for i in free:
            more = min(limit - counts[i], max(1, left * loads[i] // pool), surplus)
            counts[i] = counts[i] + more
            surplus = surplus - more
    return np.array(counts)


def scatter_about(own_key, dims, scale, bound, shards=(), kind=jnp.bfloat16):
    array = jax.random.normal(own_key, dims, jnp.float32) * scale
    if len(shards) > 0:
        array = level_of(own_key, dims, shards, -0.22, 0.18) * array
    return jnp.clip(array, min=-bound, max=bound).astype(kind)


def noise_with(stream_key, dims, scale, limit, cuts, heavy, held_as=jnp.bfloat16):
    array = scale * jax.random.normal(stream_key, dims, jnp.float32)
    if cuts:
        array = array * level_of(stream_key, dims, cuts, -0.22, 0.18)
    return jnp.clip(strengthened(array, jax.random.fold_in(stream_key, 3), *heavy), -limit, limit).astype(held_as)


def setup_inputs(seed: int = 0) -> dict:
    keys = jax.random.split(jax.random.key(seed), 17)
    mixer_out = draw_mixer_out(jax.random.fold_in(keys[16], 71), 0)
    layer_grad = noise_with(keys[1], (TOKENS, D), 1.0, 6.0, ((0, 32), (1, 16)), (0, 1, 32, 2.75))
    row_scale = jnp.clip(jnp.exp(math.log(3.0) - 2.3025851 * jax.random.uniform(keys[2], (TOKENS,), jnp.float32) ** level_of(keys[2], (TOKENS,), ((0, 32),), -0.2, 0.2)), 0.3, 3.0)
    norm_gain = jnp.clip(1.0 + 0.18 * jax.random.normal(keys[3], (D,), jnp.float32), 0.099609375, 1.8984375).astype(jnp.bfloat16)
    routes_keys = jax.random.split(jax.random.fold_in(keys[4], 1), TOKENS // TOK_DEV)
    routes_turns = jax.random.permutation(jax.random.fold_in(keys[4], 3), TOKENS // TOK_DEV)
    routes = jax.vmap(lambda own, number: routed_block(jax.random.fold_in(keys[4], 2), own, number, TOK_DEV, EXPERTS, TOP, CAP, 1))(routes_keys, routes_turns).reshape((TOKENS, TOP))
    route_weight = jnp.clip(0.05 + 0.29999999 * jax.random.uniform(keys[5], (TOKENS, TOP), jnp.float32) ** level_of(keys[5], (TOKENS, TOP), ((0, 32),), -0.2, 0.2), 0.05, 0.35)
    expert_gate = scatter_about(keys[6], (EXPERTS, FF, D), D ** -0.5, 0.125, ((0, 32), (1, 16)))
    expert_up = scatter_about(keys[7], (EXPERTS, FF, D), D ** -0.5, 0.125, ((0, 32), (1, 16)))
    expert_down = scatter_about(keys[8], (EXPERTS, FF, D), FF ** -0.5, 0.09375, ((0, 32), (1, 16)))
    query_rows = scatter_about(keys[9], (TOKENS, RET_W), 1.0, 6.0, ((0, 32), (1, 16)))
    key_rows = scatter_about(keys[10], (TOKENS, RET_W), 1.0, 6.0, ((0, 32), (1, 16)))
    value_rows = scatter_about(keys[11], (TOKENS, RET_W), 1.0, 6.0, ((0, 32), (1, 16)))
    retained = scatter_about(keys[12], (TOKENS, RET_W), 1.0, 6.0, ((0, 32), (1, 16)))
    log_decay = draw_log_decay(jax.random.fold_in(keys[16], 71), 0)
    entry_state = scatter_about(keys[14], (N_SP, HEADS, HEAD_DIM, HEAD_DIM), 2.0, 12.0, ((0, 32), (1, 16)), jnp.float32)
    out_proj = scatter_about(keys[15], (RET_W, D), RET_W ** -0.5, 0.1875, ((0, 16),))
    return dict(mixer_out=mixer_out, layer_grad=layer_grad, row_scale=row_scale, norm_gain=norm_gain, routes=routes, route_weight=route_weight, expert_gate=expert_gate, expert_up=expert_up, expert_down=expert_down, query_rows=query_rows, key_rows=key_rows, value_rows=value_rows, retained=retained, log_decay=log_decay, entry_state=entry_state, out_proj=out_proj)


def span_terms(head_queries, head_keys, head_values, head_gradient, decay_head, incoming_state):
    scale = head_queries.shape[-1] ** -0.5
    length = decay_head.shape[1]
    cumul = jnp.cumsum(decay_head, axis=1)
    places = jnp.arange(length)
    causal = (places[:, None] >= places[None, :])[None, :, :]
    spread = cumul[:, :, None] - cumul[:, None, :]
    weights = jnp.where(causal, jnp.exp(jnp.where(causal, spread, 0.0)), 0.0)
    scores = scale * jnp.einsum("thd,shd->hts", head_queries, head_keys, precision=lax.Precision.HIGHEST) * weights
    pressure = scale * jnp.einsum("thd,shd->hts", head_gradient, head_values, precision=lax.Precision.HIGHEST) * weights
    grad_query = jnp.einsum("hts,shd->thd", pressure, head_keys, precision=lax.Precision.HIGHEST)
    grad_key = jnp.einsum("hts,thd->shd", pressure, head_queries, precision=lax.Precision.HIGHEST)
    grad_value = jnp.einsum("hts,thd->shd", scores, head_gradient, precision=lax.Precision.HIGHEST)
    ascending_decay = jnp.exp(cumul).T
    grad_query = grad_query + scale * ascending_decay[:, :, None] * jnp.einsum(
        "joy,oiy->joi", head_gradient, incoming_state, precision=lax.Precision.HIGHEST)
    state_update = jnp.einsum("olb,oli->lbi", head_queries * ascending_decay[:, :, None], head_gradient, precision=lax.Precision.HIGHEST)
    survive = jnp.exp(cumul[:, -1])
    falling = jnp.exp(cumul[:, -1:] - cumul).T
    return grad_query, grad_key, grad_value, state_update, survive, falling


def add_carried(grad_key, grad_value, head_keys, head_values, falling, carried_over_state):
    scale = head_keys.shape[-1] ** -0.5
    grad_key = grad_key + scale * falling[:, :, None] * jnp.einsum(
        "upy,ruy->rup", carried_over_state, head_values, precision=lax.Precision.HIGHEST)
    grad_value = grad_value + scale * falling[:, :, None] * jnp.einsum(
        "rzw,erz->erw", carried_over_state, head_keys, precision=lax.Precision.HIGHEST)
    return grad_key, grad_value


def reference(mixer_out, layer_grad, row_scale, norm_gain, routes, route_weight, expert_gate, expert_up,
              expert_down, query_rows, key_rows, value_rows, retained, log_decay, entry_state, out_proj):
    scaled = mixer_out.astype(jnp.float32) * row_scale[:, None]
    gain_all = norm_gain.astype(jnp.float32)
    normed = (scaled * gain_all[None, :]).astype(jnp.bfloat16)
    weighted = (route_weight[:, :, None] * layer_grad.astype(jnp.float32)[:, None, :]).astype(jnp.bfloat16)
    flat_normed = jnp.concatenate([jnp.repeat(normed, TOP, axis=0), jnp.zeros((1, D), jnp.bfloat16)], axis=0)
    flat_grad = jnp.concatenate([weighted.reshape(TOKENS * TOP, D), jnp.zeros((1, D), jnp.bfloat16)], axis=0)

    blocks = routes.reshape(N_SP, TOP * TOK_DEV)
    onehot = (blocks[:, :, None] == jnp.arange(EXPERTS, dtype=jnp.int32)[None, None, :]).astype(jnp.int32)
    rank_in = jnp.sum(onehot * (jnp.cumsum(onehot, axis=1) - 1), axis=2)
    source_ids = jnp.arange(N_SP, dtype=jnp.int32)[:, None]
    position = (blocks * (N_SP * CAP) + source_ids * CAP + rank_in).reshape(-1).astype(jnp.int32)
    table = jnp.full((EXPERTS * N_SP * CAP,), TOP * TOKENS, jnp.int32)
    table = table.at[position].set(jnp.arange(TOP * TOKENS, dtype=jnp.int32)).reshape(EXPERTS, N_SP * CAP)

    width = FF // N_TP

    def expert(inputs):
        row_ids, gate_weight, up_weight, down_weight = inputs
        normed_rows = jnp.take(flat_normed, row_ids, axis=0)
        grad_rows = jnp.take(flat_grad, row_ids, axis=0)
        gate_pre = jnp.dot(normed_rows, gate_weight.T, preferred_element_type=jnp.float32)
        up_pre = jnp.dot(normed_rows, up_weight.T, preferred_element_type=jnp.float32)
        sigmoid_gate = jax.nn.sigmoid(gate_pre)
        silu_gate = gate_pre * sigmoid_gate
        activation = (silu_gate * up_pre).astype(jnp.bfloat16)
        grad_down = jnp.dot(activation.T, grad_rows, preferred_element_type=jnp.float32).astype(jnp.bfloat16)
        act_grad = jnp.dot(grad_rows, down_weight.T, preferred_element_type=jnp.float32)
        up_grad = (act_grad * silu_gate).astype(jnp.bfloat16)
        gate_grad = (act_grad * up_pre * sigmoid_gate * (1.0 + gate_pre * (1.0 - sigmoid_gate))).astype(jnp.bfloat16)
        grad_up = jnp.dot(up_grad.T, normed_rows, preferred_element_type=jnp.float32).astype(jnp.bfloat16)

        def group(index, total):
            start = (index * width).astype(jnp.int32)
            part = jnp.dot(lax.dynamic_slice_in_dim(gate_grad, start, width, 1),
                           lax.dynamic_slice_in_dim(gate_weight, start, width, 0),
                           preferred_element_type=jnp.float32)
            part = part + jnp.dot(lax.dynamic_slice_in_dim(up_grad, start, width, 1),
                                  lax.dynamic_slice_in_dim(up_weight, start, width, 0),
                                  preferred_element_type=jnp.float32)
            return total + lax.optimization_barrier(part.astype(jnp.bfloat16)).astype(jnp.float32)

        summed = lax.fori_loop(0, N_TP, group, jnp.zeros((N_SP * CAP, D), jnp.float32))
        return grad_up, grad_down, summed.astype(jnp.bfloat16)

    grad_up, grad_down, returned = lax.map(expert, (table, expert_gate, expert_up, expert_down))
    per_route = jnp.take(returned.reshape(EXPERTS * N_SP * CAP, D), position, axis=0)
    hidden_grad = jnp.sum(per_route.reshape(TOKENS, TOP, D).astype(jnp.float32), axis=1).astype(jnp.bfloat16)

    attend = gain_all[None, :] * hidden_grad.astype(jnp.float32)
    mean_dot = jnp.mean(scaled * attend, axis=1, keepdims=True)
    stream = layer_grad.astype(jnp.float32) + row_scale[:, None] * (attend - scaled * mean_dot)
    stream_grad = stream.astype(jnp.bfloat16)
    grad_proj = jnp.dot(stream_grad.T, retained, preferred_element_type=jnp.float32)
    out_grad = jnp.dot(stream_grad, out_proj.T, preferred_element_type=jnp.float32).astype(jnp.bfloat16)

    def split_heads(block):
        return block.astype(jnp.float32).reshape(N_SP, TOK_DEV, HEADS, HEAD_DIM)

    decay_spans = log_decay.reshape(HEADS, N_SP, TOK_DEV).transpose(1, 0, 2)

    def span_step(carried_over_state, pieces):
        head_queries, head_keys, head_values, head_gradient, decay_head, incoming_state = pieces
        grad_query, grad_key, grad_value, state_update, survive, falling = span_terms(
            head_queries, head_keys, head_values, head_gradient, decay_head, incoming_state)
        grad_key, grad_value = add_carried(grad_key, grad_value, head_keys, head_values, falling, carried_over_state)
        return state_update + survive[:, None, None] * carried_over_state, (grad_query, grad_key, grad_value)

    start_state = jnp.zeros((HEADS, HEAD_DIM, HEAD_DIM), jnp.float32)
    _, (grad_query, grad_key, grad_value) = lax.scan(
        span_step, start_state,
        (split_heads(query_rows), split_heads(key_rows), split_heads(value_rows), split_heads(out_grad),
         decay_spans, entry_state), reverse=True)
    ret_width = HEADS * HEAD_DIM
    return (grad_up, grad_down, grad_proj,
            grad_query.reshape(TOKENS, ret_width).astype(jnp.bfloat16),
            grad_key.reshape(TOKENS, ret_width).astype(jnp.bfloat16),
            grad_value.reshape(TOKENS, ret_width).astype(jnp.bfloat16),
            stream_grad)
```

```python
import functools

import jax
import jax.numpy as jnp
from jax import lax
from jax.experimental import pallas as pl
from jax.experimental.pallas import tpu as pltpu
from jax.sharding import PartitionSpec as P

MESH = pl.DeviceIdType.MESH
F32, BF16 = jnp.float32, jnp.bfloat16
NN = (((1,), (0,)), ((), ()))
NT = (((1,), (1,)), ((), ()))
TN = (((0,), (0,)), ((), ()))


def dot(a, b, dims=NN):
    return lax.dot_general(a, b, dims, preferred_element_type=F32)


def exact(a, b, dims=NN):
    return lax.dot_general(
        a, b, dims, precision=lax.Precision.HIGHEST, preferred_element_type=F32
    )


def iota(shape, dim):
    return lax.broadcasted_iota(jnp.int32, shape, dim)


def packed(square):
    half = square.shape[0] // 2
    return jnp.concatenate([square[:half], square[half:]], axis=1)


def unpacked(rows):
    half = rows.shape[1] // 2
    return jnp.concatenate([rows[:, :half], rows[:, half:]], axis=0)


def body_kernel(
    nz,
    nx,
    ny,
    mix,
    lgr,
    rsc,
    gain,
    routes,
    rweight,
    gate_h,
    up_h,
    down_h,
    query,
    key,
    value,
    retained,
    decay,
    entry,
    oproj,
    gup_h,
    gdown_h,
    gproj,
    gquery,
    gkey,
    gvalue,
    sgrad,
    wg,
    wu,
    wd,
    w_sem,
    disp,
    ag,
    slots,
    slots_t,
    bbuf,
    abuf,
    afull,
    cbuf,
    scores,
    decays,
    crow,
    pre_g,
    pre_u,
    pre_a,
    gg,
    ug,
    act_t,
    ug_t,
    part,
    xs,
    xr,
    scw,
    rcw,
    sccw,
    rccw,
    route,
    back,
    dots,
    sfull,
    gdown,
    gup,
    o_sem,
    ubuf,
    gps,
    gpr,
    d_s,
    d_r,
    c_s,
    c_r,
    b_s,
    b_r,
    bp_s,
    bp_r,
    ag_s,
    ag_r,
    agp_s,
    agp_r,
    x_s,
    x_r,
    rs_s,
    rs_r,
    t_s,
    t_r,
    a_s,
    a_r,
    ap_s,
    ap_r,
    p_s,
    p_r,
    u_s,
    u_r,
    g_s,
    g_r,
):
    nsp, ntp, far = nz * nx, 2 * ny, ny // 2
    tokens, cols = mix.shape
    nslots = slots.shape[0]
    cap = nslots // nsp
    half = nsp // 2
    hrows = nslots // 2
    scale = query.shape[0] ** -0.5
    me = lax.axis_index("sp")
    tp = lax.axis_index("tp")
    z, x = me // nx, me % nx
    y, c = tp // 2, tp % 2
    partner = (me, tp + 1 - 2 * c)
    up_dev = (me, lax.rem(y + 1, ny) * 2 + c)
    dn_dev = (me, lax.rem(y + ny - 1, ny) * 2 + c)

    def wrap(v, n):
        return lax.rem(v + 2 * n, n)

    def offset(k):
        i, dx = k // nx, lax.rem(k, nx)
        dz = ((i + 1) // 2) * (2 * lax.rem(i, 2) - 1)
        return dz, dx

    def source(k):
        dz, dx = offset(k)
        return wrap(z + dz, nz) * nx + wrap(x + dx, nx)

    def target(k):
        dz, dx = offset(k)
        return wrap(z - dz, nz) * nx + wrap(x - dx, nx)

    def rcopy(src, dst, ssem, rsem, dev):
        return pltpu.make_async_remote_copy(
            src_ref=src,
            dst_ref=dst,
            send_sem=ssem,
            recv_sem=rsem,
            device_id=dev,
            device_id_type=MESH,
        )

    def loop(lo, hi, fn):
        def step(i, carry):
            fn(i)
            return carry

        lax.fori_loop(lo, hi, step, 0)

    barrier = pltpu.get_barrier_semaphore()

    def greet_sp(i):
        pl.semaphore_signal(
            barrier, inc=1, device_id=(lax.rem(me + i, nsp), tp), device_id_type=MESH
        )

    def greet_tp(i):
        pl.semaphore_signal(
            barrier, inc=1, device_id=(me, lax.rem(tp + i, ntp)), device_id_type=MESH
        )

    loop(1, nsp, greet_sp)
    loop(1, ntp, greet_tp)
    loads = [
        pltpu.make_async_copy(src.at[0], dst, w_sem.at[i])
        for i, (src, dst) in enumerate(((gate_h, wg), (up_h, wu), (down_h, wd)))
    ]
    for load in loads:
        load.start()

    rs_col = jnp.transpose(jnp.broadcast_to(rsc[...], (tokens, tokens)))[:, :1]
    gain_row = jnp.sum(
        jnp.where(iota(gain.shape, 0) == tp, gain[...].astype(F32), 0.0), axis=0, keepdims=True
    )
    scaled = mix[...].astype(F32) * rs_col
    normed = (scaled * gain_row).astype(BF16)
    named = iota((nsp, tokens), 0)
    first = routes[0:1, :] == named
    second = routes[1:2, :] == named
    either = jnp.where(first | second, 1.0, 0.0)
    before = jnp.where(
        iota((tokens, tokens), 0) < iota((tokens, tokens), 1), 1.0, 0.0
    )
    rank = dot(either.astype(BF16), before.astype(BF16))
    spread = jnp.where(iota((nslots, nsp), 0) // cap == iota((nslots, nsp), 1), 1.0, 0.0)
    spread = spread.astype(BF16)
    place = lax.rem(iota((nslots, tokens), 0), cap).astype(F32)
    hit0 = dot(spread, jnp.where(first, rank, -1.0).astype(BF16)) == place
    hit1 = dot(spread, jnp.where(second, rank, -1.0).astype(BF16)) == place
    hits = jnp.where(hit0 | hit1, 1.0, 0.0)
    weight = jnp.where(hit0, rweight[0:1, :], 0.0) + jnp.where(hit1, rweight[1:2, :], 0.0)
    slot_weight = jnp.sum(weight, axis=1, keepdims=True)
    slots[...] = hits.astype(BF16)
    rows_n = dot(slots[...], normed).astype(BF16)
    rows_g = (dot(slots[...], lgr[...]) * slot_weight).astype(BF16)
    disp[:, 0:cap, :] = rows_n.reshape(nsp, cap, cols)
    disp[:, cap : 2 * cap, :] = rows_g.reshape(nsp, cap, cols)
    ag[y, c, 0] = disp[me]
    bbuf[y, c] = (scaled * rs_col).astype(BF16)

    incl = iota((tokens, tokens), 1) <= iota((tokens, tokens), 0)
    c_col = jnp.sum(
        jnp.where(incl, jnp.broadcast_to(decay[...], (tokens, tokens)), 0.0),
        axis=1,
        keepdims=True,
    )
    c_all = jnp.sum(decay[...], axis=1, keepdims=True)
    cbuf[me] = jnp.broadcast_to(c_all, cbuf.shape[1:])

    pl.semaphore_wait(barrier, nsp + ntp - 2)

    def send_rows(k):
        dev = target(k)
        rcopy(disp.at[dev], ag.at[y, c, k], d_s.at[k], d_r.at[k], (dev, tp)).start()

    def wait_rows(k):
        rcopy(disp.at[me], ag.at[y, c, k], d_s.at[k], d_r.at[k], (source(k), tp)).wait_recv()

    loop(1, nsp, send_rows)

    def peer(i):
        return (me, lax.rem(y + i, ny) * 2 + c)

    def send_b(i):
        rcopy(bbuf.at[y, c], bbuf.at[y, c], b_s.at[i], b_r.at[i], peer(i)).start()

    loop(1, ny, send_b)

    def send_c(d):
        rcopy(cbuf.at[me], cbuf.at[me], c_s.at[d], c_r.at[me], (d, tp)).start()

    loop(0, me, send_c)

    c_cols = jnp.broadcast_to(c_col, (tokens, tokens))
    c_rows = jnp.transpose(c_cols)
    gap = jnp.where(incl, c_cols - c_rows, 0.0)
    decays[...] = jnp.where(incl, jnp.exp(gap), 0.0)
    scores[...] = scale * dot(query[...], key[...], TN) * decays[...]
    crow[...] = c_rows[0:8, :]
    slots_t[...] = jnp.transpose(slots[...].astype(F32)).astype(BF16)
    pre_g[...] = jnp.zeros_like(pre_g)
    pre_u[...] = jnp.zeros_like(pre_u)
    pre_a[...] = jnp.zeros_like(pre_a)

    def yat(d):
        return wrap(y + d, ny)

    def part_of(yy, h):
        return ag.at[yy, c, pl.ds(h * half, half)]

    def ring(dirn, d, h):
        yy = yat(-d) if dirn == 0 else yat(d)
        dev = up_dev if dirn == 0 else dn_dev
        i = (dirn * far + d) * 2 + h
        return rcopy(part_of(yy, h), part_of(yy, h), ag_s.at[i], ag_r.at[i], dev)

    def arrived(dirn, d, h):
        yy = yat(-d) if dirn == 0 else yat(d)
        i = (dirn * far + d - 1) * 2 + h
        return rcopy(part_of(yy, h), part_of(yy, h), ag_s.at[i], ag_r.at[i], up_dev)

    def pair(rel, h):
        yy = yat(rel)
        i = lax.rem(rel + ny, ny) * 2 + h
        return rcopy(part_of(yy, h), part_of(yy, h), agp_s.at[i], agp_r.at[i], partner)

    def pair_in(rel, h):
        yy = yat(rel)
        i = lax.rem(rel + ny, ny) * 2 + h
        dst = ag.at[yy, 1 - c, pl.ds(h * half, half)]
        return rcopy(dst, dst, agp_s.at[i], agp_r.at[i], partner)

    def sends(dirn, d, h):
        return d < far - 1 or (d == far - 1 and h == dirn)

    def span_of(yy):
        return pl.ds(pl.multiple_of(yy * 2 * cols, 2 * cols), 2 * cols)

    def rows_of(yy, lo):
        return jnp.concatenate(
            [ag[yy, cc, :, lo : lo + cap, :].reshape(nslots, cols) for cc in range(2)], axis=1
        )

    def multiply(rel):
        yy = yat(rel)
        for h in range(2):
            pair_in(rel, h).wait_recv()
        cut = span_of(yy)
        rows_n, rows_g = rows_of(yy, 0), rows_of(yy, cap)
        pre_g[...] += dot(rows_n, wg[:, cut], NT)
        pre_u[...] += dot(rows_n, wu[:, cut], NT)
        pre_a[...] += dot(rows_g, wd[:, cut], NT)

    for h in range(2):
        loop(max(h * half, 1), (h + 1) * half, wait_rows)
        ring(0, 0, h).start()
        ring(1, 0, h).start()
        pair(0, h).start()
    for load in loads:
        load.wait()
    for d in range(1, far):
        for h in range(2):
            for dirn in range(2):
                arrived(dirn, d, h).wait_recv()
                if sends(dirn, d, h):
                    ring(dirn, d, h).start()
                pair(-d if dirn == 0 else d, h).start()
            if d == 1 and h == 0:
                multiply(0)
            elif d > 1:
                multiply(-(d - 1) if h == 0 else d - 1)
    for h in range(2):
        arrived(h, far, h).wait_recv()
        pair(far, h).start()
        if far > 1:
            multiply(-(far - 1) if h == 0 else far - 1)
        else:
            if h == 0:
                multiply(0)
    multiply(far)

    gate_pre, up_pre, act_grad = pre_g[...], pre_u[...], pre_a[...]
    sig = 1.0 / (1.0 + jnp.exp(-gate_pre))
    silu = gate_pre * sig
    ug32 = act_grad * silu
    ug[...] = ug32.astype(BF16)
    gg[...] = (act_grad * up_pre * sig * (1.0 + gate_pre * (1.0 - sig))).astype(BF16)

    def partial(rel):
        yy = yat(rel)
        cut = span_of(yy)
        both = dot(gg[...], wg[:, cut]) + dot(ug[...], wu[:, cut])
        lo, hi = both[:, :cols], both[:, cols:]
        i = lax.rem(rel + ny, ny)
        part[i] = jnp.where(c == 0, lo, hi)
        xs[i] = jnp.where(c == 0, hi, lo).astype(BF16)
        rcopy(xs.at[i], xr.at[i], x_s.at[i], x_r.at[i], partner).start()

    def joined(rel):
        i = lax.rem(rel + ny, ny)
        rcopy(xs.at[i], xr.at[i], x_s.at[i], x_r.at[i], partner).wait_recv()
        part[i] = part[i] + xr[i].astype(F32)

    def hs(h):
        return pl.ds(h * hrows, hrows)

    stage, land = (scw, sccw), (rcw, rccw)

    def pass_on(dirn, d, h, add):
        rel = d if dirn == 0 else ny - d
        rel = rel % ny
        total = part[rel, h * hrows : (h + 1) * hrows, :]
        if add:
            from_ring(dirn, d + 1, h).wait_recv()
            total = total + land[dirn][d, h * hrows : (h + 1) * hrows, :].astype(F32)
        stage[dirn][d - 1, h * hrows : (h + 1) * hrows, :] = total.astype(BF16)
        to_ring(dirn, d, h).start()

    def to_ring(dirn, d, h):
        i = (dirn * far + d - 1) * 2 + h
        return rcopy(
            stage[dirn].at[d - 1, hs(h)],
            land[dirn].at[d - 1, hs(h)],
            rs_s.at[i],
            rs_r.at[i],
            up_dev if dirn == 0 else dn_dev,
        )

    from_ring = to_ring

    grads = []

    def weight_grads(i):
        cut = span_of(i)
        gdown[:, cut] = dot(act_t[...], rows_of(i, cap)).astype(BF16)
        gup[:, cut] = dot(ug_t[...], rows_of(i, 0)).astype(BF16)

    pending = list(range(ny))

    def some_grads(n):
        for _ in range(min(n, len(pending))):
            weight_grads(pending.pop(0))

    partial(far)
    if far > 1:
        partial(far - 1)
        partial(ny - far + 1)
    joined(far)
    pass_on(0, far, 0, False)
    pass_on(1, far, 1, False)
    for d in range(far - 2, 0, -1):
        partial(d)
        partial(ny - d)
        joined(d + 1)
        joined(ny - d - 1)
        if d == far - 2:
            pass_on(0, far - 1, 1, False)
            pass_on(1, far - 1, 0, False)
    partial(0)
    if far > 1:
        joined(1)
        joined(ny - 1)
    if far == 2:
        pass_on(0, 1, 1, False)
        pass_on(1, 1, 0, False)
    act_t[...] = jnp.transpose(silu * up_pre).astype(BF16)
    ug_t[...] = jnp.transpose(ug32).astype(BF16)
    joined(0)
    if far > 1:
        pass_on(0, far - 1, 0, True)
        pass_on(1, far - 1, 1, True)
        some_grads(2)
    for d in range(far - 2, 0, -1):
        pass_on(0, d, 1, True)
        pass_on(1, d, 0, True)
        some_grads(1)
        pass_on(0, d, 0, True)
        pass_on(1, d, 1, True)
        some_grads(2)

    def send_back(k):
        rcopy(
            route.at[k], back.at[me], t_s.at[k], t_r.at[me], (source(k), tp)
        ).start()

    def wait_back(i):
        e = lax.rem(me + i, nsp)
        rcopy(route.at[0], back.at[e], t_s.at[i], t_r.at[e], (e, tp)).wait_recv()

    for h in (1, 0):
        total = part[0, h * hrows : (h + 1) * hrows, :]
        for dirn in range(2):
            if far > 1 or h == dirn:
                from_ring(dirn, 1, h).wait_recv()
                total = total + land[dirn][0, h * hrows : (h + 1) * hrows, :].astype(F32)
        route[h * half : (h + 1) * half] = total.astype(BF16).reshape(half, cap, cols)
        loop(max(h * half, 1), (h + 1) * half, send_back)
    back[me] = route[0]
    some_grads(ny)
    outs = [
        pltpu.make_async_copy(gup, gup_h.at[0], o_sem.at[0]),
        pltpu.make_async_copy(gdown, gdown_h.at[0], o_sem.at[1]),
    ]
    for out in outs:
        out.start()

    def b_pair(i):
        yy = lax.rem(y + i, ny)
        return rcopy(bbuf.at[yy, c], bbuf.at[yy, c], bp_s.at[i], bp_r.at[i], partner)

    def b_pair_in(i):
        yy = lax.rem(y + i, ny)
        return rcopy(bbuf.at[yy, 1 - c], bbuf.at[yy, 1 - c], bp_s.at[i], bp_r.at[i], partner)

    def relay_b(i):
        yy = lax.rem(y + i, ny)
        rcopy(bbuf.at[yy, c], bbuf.at[yy, c], b_s.at[i], b_r.at[ny - i], peer(i)).wait_recv()
        b_pair(i).start()

    b_pair(0).start()
    loop(1, ny, relay_b)
    loop(0, ny, lambda i: b_pair_in(i).wait_recv())

    loop(1, nsp, wait_back)
    hidden = dot(slots_t[...], back[...].reshape(nslots, cols)).astype(BF16).astype(F32)
    attend = gain_row * hidden
    rs_col = jnp.transpose(jnp.broadcast_to(rsc[...], (tokens, tokens)))[:, :1]
    scaled = mix[...].astype(F32) * rs_col
    a32 = lgr[...].astype(F32) + rs_col * attend
    afull[...] = a32
    abuf[y, c] = a32.astype(BF16)
    some = jnp.sum(scaled * attend, axis=1, keepdims=True)
    dots[tp] = jnp.transpose(jnp.broadcast_to(some, (tokens, tokens)))[0:8, :]

    def send_dot(i):
        dev = (me, lax.rem(tp + i, ntp))
        rcopy(dots.at[tp], dots.at[tp], p_s.at[i], p_r.at[i], dev).start()

    def wait_dot(i):
        other = lax.rem(tp + ntp - i, ntp)
        rcopy(dots.at[other], dots.at[other], p_s.at[i], p_r.at[i], (me, other)).wait_recv()

    def send_a(i):
        rcopy(abuf.at[y, c], abuf.at[y, c], a_s.at[i], a_r.at[i], peer(i)).start()

    def a_pair(i):
        yy = lax.rem(y + i, ny)
        return rcopy(abuf.at[yy, c], abuf.at[yy, c], ap_s.at[i], ap_r.at[i], partner)

    def a_pair_in(i):
        yy = lax.rem(y + i, ny)
        return rcopy(abuf.at[yy, 1 - c], abuf.at[yy, 1 - c], ap_s.at[i], ap_r.at[i], partner)

    def relay_a(i):
        yy = lax.rem(y + i, ny)
        rcopy(abuf.at[yy, c], abuf.at[yy, c], a_s.at[i], a_r.at[ny - i], peer(i)).wait_recv()
        a_pair(i).start()

    loop(1, ntp, send_dot)
    order = [far]
    for d in range(far - 1, 0, -1):
        order += [d, ny - d]
    for i in order:
        send_a(i)
    a_pair(0).start()
    loop(1, ntp, wait_dot)
    mean_row = jnp.sum(jnp.sum(dots[...], axis=0), axis=0, keepdims=True) * (0.125 / (cols * ntp))
    mean_col = jnp.transpose(jnp.broadcast_to(mean_row, (tokens, tokens)))[:, :1]
    sgrad[...] = (afull[...] - (scaled * rs_col) * mean_col).astype(BF16)

    def stream(i, cc):
        yy = lax.rem(y + i, ny)
        cut = pl.ds(pl.multiple_of((yy * 2 + cc) * cols, cols), cols)
        sfull[:, cut] = (
            abuf[yy, cc].astype(F32) - bbuf[yy, cc].astype(F32) * mean_col
        ).astype(BF16)

    stream(0, c)
    for i in reversed(order):
        relay_a(i)
        stream(i, c)
    for i in [0] + order[::-1]:
        a_pair_in(i).wait_recv()
        stream(i, 1 - c)

    grad_out = dot(oproj[...], sfull[...], NT).astype(BF16)
    g32 = grad_out.astype(F32)
    rise = jnp.exp(crow[0:1, :])
    fall = jnp.exp(c_all - crow[0:1, :])
    update = exact(query[...].astype(F32) * rise, g32, NT)
    ubuf[me] = packed(update).astype(BF16)

    def send_u(d):
        rcopy(ubuf.at[me], ubuf.at[me], u_s.at[d], u_r.at[me], (d, tp)).start()

    loop(0, me, send_u)

    dim = retained.shape[0]
    proj = dot(retained[...], sfull[...])
    low = iota((dim // 2, 2 * dim), 1) < dim
    for j in range(nsp // 2):
        tile = proj[:, j * 2 * dim : (j + 1) * 2 * dim]
        turned = pltpu.roll(tile, dim, 1)
        gps[2 * j] = jnp.where(low, tile[: dim // 2], turned[dim // 2 :]).astype(BF16)
        gps[2 * j + 1] = jnp.where(low, turned[: dim // 2], tile[dim // 2 :]).astype(BF16)

    def send_g(k):
        dev = target(k)
        rcopy(gps.at[dev], gpr.at[k], g_s.at[k], g_r.at[k], (dev, tp)).start()

    loop(1, nsp, send_g)
    gpr[0] = gps[me]

    q32, k32, v32 = query[...].astype(F32), key[...].astype(F32), value[...].astype(F32)
    press = scale * dot(grad_out, value[...], TN) * decays[...]
    gquery[...] = (
        exact(k32, press, NT) + scale * rise * exact(entry[0, 0], g32)
    ).astype(BF16)
    grad_key = exact(q32, press)
    grad_value = exact(g32, scores[...])

    def fold(i, carried):
        m = nsp - 1 - i
        rcopy(cbuf.at[m], cbuf.at[m], c_s.at[m], c_r.at[m], (m, tp)).wait_recv()
        rcopy(ubuf.at[m], ubuf.at[m], u_s.at[m], u_r.at[m], (m, tp)).wait_recv()
        return ubuf[m].astype(F32) + jnp.exp(cbuf[m][0:1, :]) * carried

    carried = unpacked(
        lax.fori_loop(0, nsp - 1 - me, fold, jnp.zeros((dim // 2, 2 * dim), F32))
    )
    gkey[...] = (grad_key + scale * fall * exact(carried, v32)).astype(BF16)
    gvalue[...] = (grad_value + scale * fall * exact(carried, k32, TN)).astype(BF16)

    def wait_g(k):
        rcopy(gps.at[me], gpr.at[k], g_s.at[k], g_r.at[k], (source(k), tp)).wait_recv()

    loop(1, nsp, wait_g)
    gproj[...] = jnp.transpose(unpacked(jnp.sum(gpr[...].astype(F32), axis=0)))

    def sent_sp(k):
        rcopy(disp.at[me], ag.at[y, c, k], d_s.at[k], d_r.at[k], (source(k), tp)).wait_send()
        rcopy(route.at[k], back.at[me], t_s.at[k], t_r.at[k], (source(k), tp)).wait_send()
        rcopy(gps.at[me], gpr.at[k], g_s.at[k], g_r.at[k], (source(k), tp)).wait_send()

    loop(1, nsp, sent_sp)

    def sent_early(d):
        rcopy(cbuf.at[me], cbuf.at[me], c_s.at[d], c_r.at[me], (d, tp)).wait_send()
        rcopy(ubuf.at[me], ubuf.at[me], u_s.at[d], u_r.at[me], (d, tp)).wait_send()

    loop(0, me, sent_early)

    def sent_y(i):
        rcopy(bbuf.at[y, c], bbuf.at[y, c], b_s.at[i], b_r.at[i], peer(i)).wait_send()
        rcopy(abuf.at[y, c], abuf.at[y, c], a_s.at[i], a_r.at[i], peer(i)).wait_send()

    loop(1, ny, sent_y)

    def sent_pair(i):
        b_pair(i).wait_send()
        a_pair(i).wait_send()
        for h in range(2):
            pair(i, h).wait_send()
        rcopy(xs.at[i], xr.at[i], x_s.at[i], x_r.at[i], partner).wait_send()

    loop(0, ny, sent_pair)

    def sent_dot(i):
        rcopy(dots.at[tp], dots.at[tp], p_s.at[i], p_r.at[i], partner).wait_send()

    loop(1, ntp, sent_dot)
    for dirn in range(2):
        for d in range(far):
            for h in range(2):
                if sends(dirn, d, h):
                    ring(dirn, d, h).wait_send()
        for d in range(1, far + 1):
            for h in range(2):
                if d < far or h == dirn:
                    to_ring(dirn, d, h).wait_send()
    for out in outs:
        out.wait()


def step(nz, nx, ny, *args):
    (mixer_out, layer_grad, row_scale, norm_gain, routes, route_weight) = args[:6]
    (gate, up, down, query, key, value, retained, decay, entry, oproj) = args[6:]
    nsp, ntp, far = nz * nx, 2 * ny, ny // 2
    tokens, cols = mixer_out.shape
    fanout = routes.shape[1]
    cap = 2 * fanout * tokens // nsp
    nslots = nsp * cap
    units, width = gate.shape[1:]
    dim = query.shape[1]
    shape_t = (dim, tokens)
    vmem = pl.BlockSpec(memory_space=pltpu.VMEM)
    hbm = pl.BlockSpec(memory_space=pl.ANY)
    shape = jax.ShapeDtypeStruct
    dma = pltpu.SemaphoreType.DMA
    vm = pltpu.VMEM
    scratch = [
        vm((units, width), BF16),
        vm((units, width), BF16),
        vm((units, width), BF16),
        dma((3,)),
        vm((nsp, 2 * cap, cols), BF16),
        vm((ny, 2, nsp, 2 * cap, cols), BF16),
        vm((nslots, tokens), BF16),
        vm((tokens, nslots), BF16),
        vm((ny, 2, tokens, cols), BF16),
        vm((ny, 2, tokens, cols), BF16),
        vm((tokens, cols), F32),
        vm((nsp, 8, 128), F32),
        vm((tokens, tokens), F32),
        vm((tokens, tokens), F32),
        vm((8, tokens), F32),
        vm((nslots, units), F32),
        vm((nslots, units), F32),
        vm((nslots, units), F32),
        vm((nslots, units), BF16),
        vm((nslots, units), BF16),
        vm((units, nslots), BF16),
        vm((units, nslots), BF16),
        vm((ny, nslots, cols), F32),
        vm((ny, nslots, cols), BF16),
        vm((ny, nslots, cols), BF16),
        vm((far, nslots, cols), BF16),
        vm((far, nslots, cols), BF16),
        vm((far, nslots, cols), BF16),
        vm((far, nslots, cols), BF16),
        vm((nsp, cap, cols), BF16),
        vm((nsp, cap, cols), BF16),
        vm((ntp, 8, 128), F32),
        vm((tokens, width), BF16),
        vm((units, width), BF16),
        vm((units, width), BF16),
        dma((2,)),
        vm((nsp, dim // 2, 2 * dim), BF16),
        vm((nsp, dim // 2, 2 * dim), BF16),
        vm((nsp, dim // 2, 2 * dim), BF16),
        dma((nsp,)),
        dma((nsp,)),
        dma((nsp,)),
        dma((nsp,)),
        dma((ny,)),
        dma((ny,)),
        dma((ny,)),
        dma((ny,)),
        dma((4 * far,)),
        dma((4 * far,)),
        dma((2 * ny,)),
        dma((2 * ny,)),
        dma((ny,)),
        dma((ny,)),
        dma((4 * far,)),
        dma((4 * far,)),
        dma((nsp,)),
        dma((nsp,)),
        dma((ny,)),
        dma((ny,)),
        dma((ny,)),
        dma((ny,)),
        dma((ntp,)),
        dma((ntp,)),
        dma((nsp,)),
        dma((nsp,)),
        dma((nsp,)),
        dma((nsp,)),
    ]
    outs = pl.pallas_call(
        functools.partial(body_kernel, nz, nx, ny),
        out_shape=(
            shape(up.shape, BF16),
            shape(down.shape, BF16),
            shape((width // nsp, dim), F32),
            shape(shape_t, BF16),
            shape(shape_t, BF16),
            shape(shape_t, BF16),
            shape(mixer_out.shape, BF16),
        ),
        in_specs=[vmem] * 6 + [hbm] * 3 + [vmem] * 7,
        out_specs=(hbm, hbm) + (vmem,) * 5,
        scratch_shapes=scratch,
        compiler_params=pltpu.CompilerParams(
            collective_id=0, has_side_effects=True, vmem_limit_bytes=60_000_000
        ),
    )(
        mixer_out,
        layer_grad,
        row_scale.reshape(1, tokens),
        norm_gain.reshape(ntp, cols),
        routes.T,
        route_weight.T,
        gate,
        up,
        down,
        query.T,
        key.T,
        value.T,
        retained.T,
        decay,
        entry,
        oproj,
    )
    return (*outs[:3], outs[3].T, outs[4].T, outs[5].T, outs[6])


def specs():
    in_specs = (
        P("sp", "tp"),
        P("sp", "tp"),
        P("sp"),
        P(),
        P("sp", None),
        P("sp", None),
        P("sp", "tp", None),
        P("sp", "tp", None),
        P("sp", "tp", None),
        P("sp", "tp"),
        P("sp", "tp"),
        P("sp", "tp"),
        P("sp", "tp"),
        P("tp", "sp"),
        P("sp", "tp", None, None),
        P("tp", None),
    )
    out_specs = (
        P("sp", "tp", None),
        P("sp", "tp", None),
        P("sp", "tp"),
        P("sp", "tp"),
        P("sp", "tp"),
        P("sp", "tp"),
        P("sp", "tp"),
    )
    return in_specs, out_specs


def solution(mesh, nx=4):
    nsp, ntp = mesh.shape["sp"], mesh.shape["tp"]
    in_specs, out_specs = specs()
    return jax.shard_map(
        functools.partial(step, nsp // nx, nx, ntp // 2),
        mesh=mesh,
        in_specs=in_specs,
        out_specs=out_specs,
        check_vma=False,
    )
```

```python
import functools

import jax
import jax.numpy as jnp
from jax import lax
from jax.experimental import pallas as pl
from jax.experimental.pallas import tpu as pltpu
from jax.sharding import PartitionSpec as P

MESH = pl.DeviceIdType.MESH
F32, BF16 = jnp.float32, jnp.bfloat16
NN = (((1,), (0,)), ((), ()))
NT = (((1,), (1,)), ((), ()))
TN = (((0,), (0,)), ((), ()))


def dot(a, b, dims=NN):
    return lax.dot_general(a, b, dims, preferred_element_type=F32)


def exact(a, b, dims=NN):
    return lax.dot_general(
        a, b, dims, precision=lax.Precision.HIGHEST, preferred_element_type=F32
    )


def iota(shape, dim):
    return lax.broadcasted_iota(jnp.int32, shape, dim)


def packed(square):
    half = square.shape[0] // 2
    return jnp.concatenate([square[:half], square[half:]], axis=1)


def unpacked(rows):
    half = rows.shape[1] // 2
    return jnp.concatenate([rows[:, :half], rows[:, half:]], axis=0)


def body_kernel(
    nz,
    nx,
    ny,
    mix_h,
    lgr_h,
    rsc_h,
    gain_h,
    routes_h,
    rweight_h,
    gate_h,
    up_h,
    down_h,
    query_h,
    key_h,
    value_h,
    retained_h,
    decay_h,
    entry_h,
    oproj_h,
    gup_h,
    gdown_h,
    gproj,
    gquery,
    gkey,
    gvalue,
    sgrad,
    mix,
    lgr,
    rsc,
    gain,
    routes,
    rweight,
    query,
    key,
    value,
    retained,
    decay,
    entry,
    oproj,
    in_sem,
    wg,
    wu,
    wd,
    w_sem,
    disp,
    ag,
    slots,
    slots_t,
    bbuf,
    abuf,
    afull,
    cbuf,
    scores,
    decays,
    crow,
    pre_g,
    pre_u,
    pre_a,
    gg,
    ug,
    act,
    act_t,
    ug_t,
    part,
    xs,
    xr,
    scw,
    rcw,
    sccw,
    rccw,
    route,
    back,
    dots,
    sfull,
    gdown,
    gup,
    o_sem,
    ubuf,
    tbuf,
    gps,
    gpr,
    d_s,
    d_r,
    c_s,
    c_r,
    b_s,
    b_r,
    bp_s,
    bp_r,
    ag_s,
    ag_r,
    agp_s,
    agp_r,
    x_s,
    x_r,
    rs_s,
    rs_r,
    t_s,
    t_r,
    a_s,
    a_r,
    ap_s,
    ap_r,
    p_s,
    p_r,
    u_s,
    u_r,
    v_s,
    v_r,
    g_s,
    g_r,
):
    nsp, ntp, far = nz * nx, 2 * ny, ny // 2
    tokens, cols = mix.shape
    nslots = slots.shape[0]
    cap = nslots // nsp
    quarter = nsp // 4
    qrows = quarter * cap
    hrows = 2 * qrows
    scale = query.shape[0] ** -0.5
    me = lax.axis_index("sp")
    tp = lax.axis_index("tp")
    z, x = me // nx, me % nx
    y, c = tp // 2, tp % 2
    partner = (me, tp + 1 - 2 * c)
    ahead = [
        [(me, lax.rem(y + (hops if dirn == 0 else ny - hops), ny) * 2 + c) for hops in range(3)]
        for dirn in range(2)
    ]

    def wrap(v, n):
        return lax.rem(v + 2 * n, n)

    def offset(k):
        i, dx = k // nx, lax.rem(k, nx)
        dz = ((i + 1) // 2) * (2 * lax.rem(i, 2) - 1)
        return dz, dx

    def source(k):
        dz, dx = offset(k)
        return wrap(z + dz, nz) * nx + wrap(x + dx, nx)

    def target(k):
        dz, dx = offset(k)
        return wrap(z - dz, nz) * nx + wrap(x - dx, nx)

    def rcopy(src, dst, ssem, rsem, dev):
        return pltpu.make_async_remote_copy(
            src_ref=src,
            dst_ref=dst,
            send_sem=ssem,
            recv_sem=rsem,
            device_id=dev,
            device_id_type=MESH,
        )

    def loop(lo, hi, fn):
        def step(i, carry):
            fn(i)
            return carry

        lax.fori_loop(lo, hi, step, 0)

    barrier = pltpu.get_barrier_semaphore()

    def greet_sp(i):
        pl.semaphore_signal(
            barrier, inc=1, device_id=(lax.rem(me + i, nsp), tp), device_id_type=MESH
        )

    def greet_tp(i):
        pl.semaphore_signal(
            barrier, inc=1, device_id=(me, lax.rem(tp + i, ntp)), device_id_type=MESH
        )

    loop(1, nsp, greet_sp)
    loop(1, ntp, greet_tp)
    brought = [
        pltpu.make_async_copy(src, dst, in_sem.at[i])
        for i, (src, dst) in enumerate(
            (
                (mix_h, mix),
                (lgr_h, lgr),
                (rsc_h, rsc),
                (gain_h, gain),
                (routes_h, routes),
                (rweight_h, rweight),
                (decay_h, decay),
                (query_h, query),
                (key_h, key),
                (value_h, value),
                (retained_h, retained),
                (entry_h, entry),
                (oproj_h, oproj),
            )
        )
    ]
    for one in brought:
        one.start()
    loads = [
        pltpu.make_async_copy(src.at[0], dst, w_sem.at[i])
        for i, (src, dst) in enumerate(((gate_h, wg), (up_h, wu), (down_h, wd)))
    ]
    for load in loads:
        load.start()

    for one in brought[:7]:
        one.wait()
    rs_col = jnp.transpose(jnp.broadcast_to(rsc[...], (tokens, tokens)))[:, :1]
    gain_row = jnp.sum(
        jnp.where(iota(gain.shape, 0) == tp, gain[...].astype(F32), 0.0), axis=0, keepdims=True
    )
    scaled = mix[...].astype(F32) * rs_col
    normed = (scaled * gain_row).astype(BF16)
    named = iota((nsp, tokens), 0)
    first = routes[0:1, :] == named
    second = routes[1:2, :] == named
    either = jnp.where(first | second, 1.0, 0.0)
    before = jnp.where(
        iota((tokens, tokens), 0) < iota((tokens, tokens), 1), 1.0, 0.0
    )
    rank = dot(either.astype(BF16), before.astype(BF16))
    spread = jnp.where(iota((nslots, nsp), 0) // cap == iota((nslots, nsp), 1), 1.0, 0.0)
    spread = spread.astype(BF16)
    place = lax.rem(iota((nslots, tokens), 0), cap).astype(F32)
    hit0 = dot(spread, jnp.where(first, rank, -1.0).astype(BF16)) == place
    hit1 = dot(spread, jnp.where(second, rank, -1.0).astype(BF16)) == place
    hits = jnp.where(hit0 | hit1, 1.0, 0.0)
    weight = jnp.where(hit0, rweight[0:1, :], 0.0) + jnp.where(hit1, rweight[1:2, :], 0.0)
    slot_weight = jnp.sum(weight, axis=1, keepdims=True)
    slots[...] = hits.astype(BF16)
    rows_n = dot(slots[...], normed).astype(BF16)
    rows_g = (dot(slots[...], lgr[...]) * slot_weight).astype(BF16)
    disp[:, 0:cap, :] = rows_n.reshape(nsp, cap, cols)
    disp[:, cap : 2 * cap, :] = rows_g.reshape(nsp, cap, cols)
    ag[y, c, 0] = disp[me]
    bbuf[y, c] = (scaled * rs_col).astype(BF16)

    incl = iota((tokens, tokens), 1) <= iota((tokens, tokens), 0)
    c_col = jnp.sum(
        jnp.where(incl, jnp.broadcast_to(decay[...], (tokens, tokens)), 0.0),
        axis=1,
        keepdims=True,
    )
    c_all = jnp.sum(decay[...], axis=1, keepdims=True)
    cbuf[me] = jnp.broadcast_to(c_all, cbuf.shape[1:])

    pl.semaphore_wait(barrier, nsp + ntp - 2)

    def send_rows(k):
        dev = target(k)
        rcopy(disp.at[dev], ag.at[y, c, k], d_s.at[k], d_r.at[k], (dev, tp)).start()

    def wait_rows(k):
        rcopy(disp.at[me], ag.at[y, c, k], d_s.at[k], d_r.at[k], (source(k), tp)).wait_recv()

    near = 2 * quarter
    loop(1, near, send_rows)

    def peer(i):
        return (me, lax.rem(y + i, ny) * 2 + c)

    def send_b(i):
        rcopy(bbuf.at[y, c], bbuf.at[y, c], b_s.at[i], b_r.at[i], peer(i)).start()

    order = [far]
    for d in range(far - 1, 0, -1):
        order += [d, ny - d]
    early = [i for i in order if min(i, ny - i) <= 2]
    late = [i for i in order if i not in early]
    for i in early:
        send_b(i)

    for one in brought[7:]:
        one.wait()
    c_cols = jnp.broadcast_to(c_col, (tokens, tokens))
    c_rows = jnp.transpose(c_cols)
    gap = jnp.where(incl, c_cols - c_rows, 0.0)
    decays[...] = jnp.where(incl, jnp.exp(gap), 0.0)
    scores[...] = scale * dot(query[...], key[...], TN) * decays[...]
    crow[...] = c_rows[0:8, :]
    slots_t[...] = jnp.transpose(slots[...].astype(F32)).astype(BF16)
    pre_g[...] = jnp.zeros_like(pre_g)
    pre_u[...] = jnp.zeros_like(pre_u)
    pre_a[...] = jnp.zeros_like(pre_a)

    def left_rows(k):
        rcopy(disp.at[me], ag.at[y, c, k], d_s.at[k], d_r.at[k], partner).wait_send()

    loop(1, near, left_rows)
    loop(near, nsp, send_rows)

    def yat(d):
        return wrap(y + d, ny)

    def part_of(yy, cc, g):
        return ag.at[yy, cc, pl.ds(g * quarter, quarter)]

    def ring(dirn, d, g, hops=1):
        piece = part_of(yat(-d) if dirn == 0 else yat(d), c, g)
        i = (dirn * far + d + hops - 1) * 4 + g
        return rcopy(piece, piece, ag_s.at[i], ag_r.at[i], ahead[dirn][hops])

    def arrived(dirn, d, g):
        piece = part_of(yat(-d) if dirn == 0 else yat(d), c, g)
        i = (dirn * far + d - 1) * 4 + g
        return rcopy(piece, piece, ag_s.at[i], ag_r.at[i], partner)

    def pair(rel, g, cc):
        piece = part_of(yat(rel), cc, g)
        i = lax.rem(rel + ny, ny) * 4 + g
        return rcopy(piece, piece, agp_s.at[i], agp_r.at[i], partner)

    def sends(dirn, d, g):
        if d < far - 1:
            return (1, 2) if d == far - 2 and g >= 2 and g % 2 == dirn else (1,)
        return (1,) if d == far - 1 and g < 2 and g % 2 == dirn else ()

    def forward(dirn, d, g):
        for hops in sends(dirn, d, g):
            ring(dirn, d, g, hops).start()

    def span_of(yy):
        return pl.ds(pl.multiple_of(yy * 2 * cols, 2 * cols), 2 * cols)

    def rows_of(yy, lo, first_slot, count):
        return jnp.concatenate(
            [
                ag[yy, cc, first_slot : first_slot + count, lo : lo + cap, :].reshape(
                    count * cap, cols
                )
                for cc in range(2)
            ],
            axis=1,
        )

    def groups(p):
        return (2 * p, 2 * p + 1)

    def multiply(p, rel):
        for g in groups(p):
            pair(rel, g, 1 - c).wait_recv()
        yy = yat(rel)
        cut = span_of(yy)
        rows = slice(p * hrows, (p + 1) * hrows)
        rows_n = rows_of(yy, 0, p * near, near)
        rows_g = rows_of(yy, cap, p * near, near)
        pre_g[rows, :] += dot(rows_n, wg[:, cut], NT)
        pre_u[rows, :] += dot(rows_n, wu[:, cut], NT)
        pre_a[rows, :] += dot(rows_g, wd[:, cut], NT)

    def own_out(p):
        for g in groups(p):
            forward(0, 0, g)
            forward(1, 0, g)
        for g in groups(p):
            pair(0, g, c).start()

    def gather_step(p, d):
        for g in groups(p):
            for dirn in range(2):
                arrived(dirn, d, g).wait_recv()
                forward(dirn, d, g)
                pair(-d if dirn == 0 else d, g, c).start()
        if d == 1:
            multiply(p, 0)
        else:
            multiply(p, 1 - d)
            multiply(p, d - 1)

    def gather_last(p):
        for g in groups(p):
            arrived(g % 2, far, g).wait_recv()
            pair(far, g, c).start()
        if far > 1:
            multiply(p, 1 - far)
            multiply(p, far - 1)
        else:
            multiply(p, 0)
        multiply(p, far)

    def pointwise(p):
        rows = slice(p * hrows, (p + 1) * hrows)
        gate_pre, up_pre, act_grad = pre_g[rows, :], pre_u[rows, :], pre_a[rows, :]
        sig = 1.0 / (1.0 + jnp.exp(-gate_pre))
        silu = gate_pre * sig
        act[rows, :] = (silu * up_pre).astype(BF16)
        ug[rows, :] = (act_grad * silu).astype(BF16)
        gg[rows, :] = (act_grad * up_pre * sig * (1.0 + gate_pre * (1.0 - sig))).astype(BF16)

    def to_pair(p, i):
        rows = pl.ds(p * hrows, hrows)
        return rcopy(
            xs.at[i, rows], xr.at[i, rows], x_s.at[2 * i + p], x_r.at[2 * i + p], partner
        )

    def partial(p, rel):
        rel = rel % ny
        rows = slice(p * hrows, (p + 1) * hrows)
        cut = span_of(yat(rel))
        both = dot(gg[rows, :], wg[:, cut]) + dot(ug[rows, :], wu[:, cut])
        lo, hi = both[:, :cols], both[:, cols:]
        part[rel, rows, :] = jnp.where(c == 0, lo, hi)
        xs[rel, rows, :] = jnp.where(c == 0, hi, lo).astype(BF16)
        to_pair(p, rel).start()

    stage, land = (scw, sccw), (rcw, rccw)

    def joined(p, rel):
        to_pair(p, rel % ny).wait_recv()

    def summed(rel, g):
        rows = slice(g * qrows, (g + 1) * qrows)
        return part[rel % ny, rows, :] + xr[rel % ny, rows, :].astype(F32)

    def hop(dirn, d, g):
        i = (dirn * far + d - 1) * 4 + g
        rows = pl.ds(g * qrows, qrows)
        return rcopy(
            stage[dirn].at[d - 1, rows],
            land[dirn].at[d - 1, rows],
            rs_s.at[i],
            rs_r.at[i],
            ahead[dirn][1 if g < 2 else d if d <= 2 else d - 2],
        )

    def taken(dirn, d, g):
        hop(dirn, d, g).wait_recv()
        return land[dirn][d - 1, g * qrows : (g + 1) * qrows, :].astype(F32)

    def hops_for(d, g):
        return [g % 2] if d == far else [0, 1]

    def push(d):
        for g in groups(1):
            for dirn in hops_for(d, g):
                total = summed(d if dirn == 0 else -d, g)
                if d == 2 and far > 2:
                    for more in range(3, far + 1):
                        if dirn in hops_for(more, g):
                            total = total + taken(dirn, more, g)
                stage[dirn][d - 1, g * qrows : (g + 1) * qrows, :] = total.astype(BF16)
                hop(dirn, d, g).start()

    def pass_on(d, dirn, g):
        total = summed(d if dirn == 0 else -d, g)
        if d < far - 1 or (d == far - 1 and g % 2 == dirn):
            total = total + taken(dirn, d + 1, g)
        stage[dirn][d - 1, g * qrows : (g + 1) * qrows, :] = total.astype(BF16)
        hop(dirn, d, g).start()

    def send_back(k):
        rcopy(
            route.at[k], back.at[me], t_s.at[k], t_r.at[me], (source(k), tp)
        ).start()

    def ring_end(p):
        for g in groups(p):
            total = summed(0, g)
            for d in (1,) if p == 0 else (1, 2):
                for dirn in hops_for(d, g):
                    total = total + taken(dirn, d, g)
            route[g * quarter : (g + 1) * quarter] = (
                total.astype(BF16).reshape(quarter, cap, cols)
            )
            loop(max(g * quarter, 1), (g + 1) * quarter, send_back)
        if p == 0:
            back[me] = route[0]

    def reduce_stages(p):
        outer = [r for d in range(far, 2, -1) for r in {d, ny - d}]
        inner = [r for d in range(min(2, far), 0, -1) for r in {d, ny - d}] + [0]
        same = [(g % 2, g) for g in groups(p)]
        other = [(1 - g % 2, g) for g in groups(p)]

        def begin():
            pointwise(p)
            for rel in outer:
                partial(p, rel)

        def second():
            for rel in outer:
                joined(p, rel)
            if p == 1:
                for d in range(far, 2, -1):
                    push(d)
            else:
                for dirn, g in same:
                    pass_on(far, dirn, g)
                for dirn, g in other:
                    pass_on(far - 1, dirn, g)

        def third():
            for rel in inner:
                partial(p, rel)

        def fourth():
            for rel in inner:
                joined(p, rel)
            if p == 1:
                push(1)
            else:
                for dirn, g in same:
                    pass_on(far - 1, dirn, g)

        def fifth():
            if p == 1:
                push(2)
            else:
                for dirn, g in other + same:
                    pass_on(2, dirn, g)

        def sixth():
            for dirn, g in other + same:
                pass_on(1, dirn, g)

        return begin, second, third, fourth, fifth, sixth, lambda: ring_end(p)

    loop(1, near, wait_rows)
    own_out(0)

    def send_c(d):
        @pl.when(d != me)
        def _():
            rcopy(cbuf.at[me], cbuf.at[me], c_s.at[d], c_r.at[me], (d, tp)).start()

    loop(0, (z + 1) * nx, send_c)
    for load in loads:
        load.wait()
    first_sum, second_sum = reduce_stages(0), reduce_stages(1)
    gather_step(0, 1)
    loop(near, nsp, wait_rows)
    own_out(1)
    for d in range(2, far):
        gather_step(0, d)
        gather_step(1, d - 1)
    gather_last(0)
    first_sum[0]()
    gather_step(1, far - 1)
    first_sum[1]()
    first_sum[2]()
    gather_last(1)
    first_sum[3]()
    second_sum[0]()
    second_sum[1]()
    first_sum[4]()
    second_sum[2]()
    second_sum[3]()
    act_t[...] = jnp.transpose(act[...].astype(F32)).astype(BF16)
    ug_t[...] = jnp.transpose(ug[...].astype(F32)).astype(BF16)

    def weight_grads(i):
        cut = span_of(i)
        gdown[:, cut] = dot(act_t[...], rows_of(i, cap, 0, nsp)).astype(BF16)
        gup[:, cut] = dot(ug_t[...], rows_of(i, 0, 0, nsp)).astype(BF16)

    pending = list(range(ny))

    def some_grads(n):
        for _ in range(min(n, len(pending))):
            weight_grads(pending.pop(0))

    some_grads(1)
    second_sum[4]()
    first_sum[5]()
    some_grads(2)
    second_sum[6]()
    some_grads(1)
    first_sum[6]()
    for i in late:
        send_b(i)

    some_grads(ny)
    outs = [
        pltpu.make_async_copy(gup, gup_h.at[0], o_sem.at[0]),
        pltpu.make_async_copy(gdown, gdown_h.at[0], o_sem.at[1]),
    ]
    for out in outs:
        out.start()

    def wait_back(i):
        e = lax.rem(me + i, nsp)
        rcopy(route.at[0], back.at[e], t_s.at[i], t_r.at[e], (e, tp)).wait_recv()

    def wait_back(i):
        e = lax.rem(me + i, nsp)
        rcopy(route.at[0], back.at[e], t_s.at[i], t_r.at[e], (e, tp)).wait_recv()

    def b_pair(i):
        yy = lax.rem(y + i, ny)
        return rcopy(bbuf.at[yy, c], bbuf.at[yy, c], bp_s.at[i], bp_r.at[i], partner)

    def b_pair_in(i):
        yy = lax.rem(y + i, ny)
        return rcopy(bbuf.at[yy, 1 - c], bbuf.at[yy, 1 - c], bp_s.at[i], bp_r.at[i], partner)

    def relay_b(i):
        yy = lax.rem(y + i, ny)
        rcopy(bbuf.at[yy, c], bbuf.at[yy, c], b_s.at[i], b_r.at[ny - i], peer(i)).wait_recv()
        b_pair(i).start()

    b_pair(0).start()
    for i in early:
        relay_b(i)

    loop(1, nsp, wait_back)
    hidden = dot(slots_t[...], back[...].reshape(nslots, cols)).astype(BF16).astype(F32)
    attend = gain_row * hidden
    rs_col = jnp.transpose(jnp.broadcast_to(rsc[...], (tokens, tokens)))[:, :1]
    scaled = mix[...].astype(F32) * rs_col
    a32 = lgr[...].astype(F32) + rs_col * attend
    afull[...] = a32
    abuf[y, c] = a32.astype(BF16)
    some = jnp.sum(scaled * attend, axis=1, keepdims=True)
    dots[tp] = jnp.transpose(jnp.broadcast_to(some, (tokens, tokens)))[0:1, :]

    def send_dot(i):
        dev = (me, lax.rem(tp + i, ntp))
        rcopy(dots.at[tp], dots.at[tp], p_s.at[i], p_r.at[i], dev).start()

    def wait_dot(i):
        other = lax.rem(tp + ntp - i, ntp)
        rcopy(dots.at[other], dots.at[other], p_s.at[i], p_r.at[i], (me, other)).wait_recv()

    def send_a(i):
        rcopy(abuf.at[y, c], abuf.at[y, c], a_s.at[i], a_r.at[i], peer(i)).start()

    def a_pair(i):
        yy = lax.rem(y + i, ny)
        return rcopy(abuf.at[yy, c], abuf.at[yy, c], ap_s.at[i], ap_r.at[i], partner)

    def a_pair_in(i):
        yy = lax.rem(y + i, ny)
        return rcopy(abuf.at[yy, 1 - c], abuf.at[yy, 1 - c], ap_s.at[i], ap_r.at[i], partner)

    def relay_a(i):
        yy = lax.rem(y + i, ny)
        rcopy(abuf.at[yy, c], abuf.at[yy, c], a_s.at[i], a_r.at[ny - i], peer(i)).wait_recv()
        a_pair(i).start()

    loop(1, ntp, send_dot)
    for i in order:
        send_a(i)
    a_pair(0).start()
    for i in late:
        relay_b(i)
    for i in range(ny):
        b_pair_in(i).wait_recv()
    loop(1, ntp, wait_dot)
    mean_row = jnp.sum(dots[...], axis=0) * (1.0 / (cols * ntp))
    mean_col = jnp.transpose(jnp.broadcast_to(mean_row, (tokens, tokens)))[:, :1]
    sgrad[...] = (afull[...] - (scaled * rs_col) * mean_col).astype(BF16)

    def stream(i, cc):
        yy = lax.rem(y + i, ny)
        cut = pl.ds(pl.multiple_of((yy * 2 + cc) * cols, cols), cols)
        sfull[:, cut] = (
            abuf[yy, cc].astype(F32) - bbuf[yy, cc].astype(F32) * mean_col
        ).astype(BF16)

    stream(0, c)
    for i in reversed(order):
        relay_a(i)
        stream(i, c)
    for i in [0] + order[::-1]:
        a_pair_in(i).wait_recv()
        stream(i, 1 - c)

    grad_out = dot(oproj[...], sfull[...], NT).astype(BF16)
    g32 = grad_out.astype(F32)
    rise = jnp.exp(crow[0:1, :])
    fall = jnp.exp(c_all - crow[0:1, :])
    update = exact(query[...].astype(F32) * rise, g32, NT)
    ubuf[x] = packed(update).astype(BF16)

    def send_u(i):
        xx = lax.rem(x + i, nx)
        rcopy(ubuf.at[x], ubuf.at[x], u_s.at[i], u_r.at[x], (z * nx + xx, tp)).start()

    def wait_u(i):
        xx = lax.rem(x + i, nx)
        rcopy(ubuf.at[xx], ubuf.at[xx], u_s.at[i], u_r.at[xx], (z * nx + xx, tp)).wait_recv()

    loop(1, nx, send_u)

    dim = retained.shape[0]
    proj = dot(retained[...], sfull[...])
    low = iota((dim // 2, 2 * dim), 1) < dim
    for j in range(nsp // 2):
        tile = proj[:, j * 2 * dim : (j + 1) * 2 * dim]
        turned = pltpu.roll(tile, dim, 1)
        gps[2 * j] = jnp.where(low, tile[: dim // 2], turned[dim // 2 :]).astype(BF16)
        gps[2 * j + 1] = jnp.where(low, turned[: dim // 2], tile[dim // 2 :]).astype(BF16)

    def send_g(k):
        dev = target(k)
        rcopy(gps.at[dev], gpr.at[k], g_s.at[k], g_r.at[k], (dev, tp)).start()

    loop(0, nsp - near, lambda i: send_g(nsp - 1 - i))

    def wait_c(i):
        m = z * nx + i

        @pl.when(m != me)
        def _():
            rcopy(cbuf.at[m], cbuf.at[m], c_s.at[m], c_r.at[m], (m, tp)).wait_recv()

    loop(0, nsp - z * nx, wait_c)
    loop(1, nx, wait_u)
    held = jnp.zeros((dim // 2, 2 * dim), F32)
    inside, after = held, jnp.zeros((1, 2 * dim), F32)
    for xx in range(nx - 1, -1, -1):
        drop = cbuf[z * nx + xx]
        inside = jnp.where(xx == x, held, inside)
        after = after + jnp.where(xx > x, drop, 0.0)
        held = ubuf[xx].astype(F32) + jnp.exp(drop) * held
    tbuf[z] = held.astype(BF16)

    def send_t(zz):
        rcopy(tbuf.at[z], tbuf.at[z], v_s.at[zz], v_r.at[z], (zz * nx + x, tp)).start()

    loop(0, z, send_t)
    loop(1, near, send_g)
    gpr[0] = gps[me]

    q32, k32, v32 = query[...].astype(F32), key[...].astype(F32), value[...].astype(F32)
    press = scale * dot(grad_out, value[...], TN) * decays[...]
    gquery[...] = (
        exact(k32, press, NT) + scale * rise * exact(entry[0, 0], g32)
    ).astype(BF16)
    grad_key = exact(q32, press)
    grad_value = exact(g32, scores[...])

    for out in outs:
        out.wait()
    def sent_sp(k):
        rcopy(route.at[k], back.at[me], t_s.at[k], t_r.at[k], (source(k), tp)).wait_send()

    loop(near, nsp, left_rows)
    loop(1, nsp, sent_sp)

    def sent_c(d):
        @pl.when(d != me)
        def _():
            rcopy(cbuf.at[me], cbuf.at[me], c_s.at[d], c_r.at[me], (d, tp)).wait_send()

    loop(0, (z + 1) * nx, sent_c)

    def sent_u(i):
        rcopy(ubuf.at[x], ubuf.at[x], u_s.at[i], u_r.at[x], partner).wait_send()

    loop(1, nx, sent_u)

    def sent_t(zz):
        rcopy(tbuf.at[z], tbuf.at[z], v_s.at[zz], v_r.at[z], partner).wait_send()

    loop(0, z, sent_t)

    def sent_y(i):
        rcopy(bbuf.at[y, c], bbuf.at[y, c], b_s.at[i], b_r.at[i], peer(i)).wait_send()
        rcopy(abuf.at[y, c], abuf.at[y, c], a_s.at[i], a_r.at[i], peer(i)).wait_send()

    loop(1, ny, sent_y)

    def sent_pair(i):
        b_pair(i).wait_send()
        a_pair(i).wait_send()
        for g in range(4):
            pair(i, g, c).wait_send()
        for p in range(2):
            to_pair(p, i).wait_send()

    loop(0, ny, sent_pair)

    def sent_dot(i):
        rcopy(dots.at[tp], dots.at[tp], p_s.at[i], p_r.at[i], partner).wait_send()

    loop(1, ntp, sent_dot)
    for g in range(4):
        for dirn in range(2):
            for d in range(far):
                for hops in sends(dirn, d, g):
                    ring(dirn, d, g, hops).wait_send()
        for d in range(1, far + 1):
            for dirn in hops_for(d, g):
                hop(dirn, d, g).wait_send()

    def fold(i, carried):
        zz = nz - 1 - i
        rcopy(tbuf.at[zz], tbuf.at[zz], v_s.at[zz], v_r.at[zz], (zz * nx + x, tp)).wait_recv()
        drop = cbuf[zz * nx]
        for xx in range(1, nx):
            drop = drop + cbuf[zz * nx + xx]
        return tbuf[zz].astype(F32) + jnp.exp(drop) * carried

    beyond = lax.fori_loop(0, nz - 1 - z, fold, jnp.zeros((dim // 2, 2 * dim), F32))
    carried = unpacked(inside + jnp.exp(after) * beyond)
    gkey[...] = (grad_key + scale * fall * exact(carried, v32)).astype(BF16)
    gvalue[...] = (grad_value + scale * fall * exact(carried, k32, TN)).astype(BF16)

    def wait_g(k):
        rcopy(gps.at[me], gpr.at[k], g_s.at[k], g_r.at[k], (source(k), tp)).wait_recv()

    loop(1, nsp, wait_g)
    gproj[...] = jnp.transpose(unpacked(jnp.sum(gpr[...].astype(F32), axis=0)))

    def sent_g(k):
        rcopy(gps.at[me], gpr.at[k], g_s.at[k], g_r.at[k], (source(k), tp)).wait_send()

    loop(1, nsp, sent_g)

def deliver(*refs):
    sources, results, held, (taken, given) = refs[:7], refs[7:14], refs[14:21], refs[21:]
    ins = [pltpu.make_async_copy(sources[i], held[i], taken.at[i]) for i in range(7)]
    copies = [pltpu.make_async_copy(held[i], results[i], given.at[i]) for i in range(7)]
    for one in ins:
        one.start()
    for one, copy in zip(ins, copies):
        one.wait()
        copy.start()
    for copy in copies:
        copy.wait()


def step(nz, nx, ny, *args):
    (mixer_out, layer_grad, row_scale, norm_gain, routes, route_weight) = args[:6]
    (gate, up, down, query, key, value, retained, decay, entry, oproj) = args[6:]
    nsp, ntp, far = nz * nx, 2 * ny, ny // 2
    tokens, cols = mixer_out.shape
    fanout = routes.shape[1]
    cap = 2 * fanout * tokens // nsp
    nslots = nsp * cap
    units, width = gate.shape[1:]
    dim = query.shape[1]
    shape_t = (dim, tokens)
    vmem = pl.BlockSpec(memory_space=pltpu.VMEM)
    hbm = pl.BlockSpec(memory_space=pltpu.HBM)
    shape = jax.ShapeDtypeStruct
    dma = pltpu.SemaphoreType.DMA
    vm = pltpu.VMEM
    scratch = [
        vm((tokens, cols), BF16),
        vm((tokens, cols), BF16),
        vm((1, tokens), F32),
        vm((ntp, cols), BF16),
        vm((fanout, tokens), jnp.int32),
        vm((fanout, tokens), F32),
        vm((dim, tokens), BF16),
        vm((dim, tokens), BF16),
        vm((dim, tokens), BF16),
        vm((dim, tokens), BF16),
        vm((1, tokens), F32),
        vm(entry.shape, F32),
        vm(oproj.shape, BF16),
        dma((13,)),
        vm((units, width), BF16),
        vm((units, width), BF16),
        vm((units, width), BF16),
        dma((3,)),
        vm((nsp, 2 * cap, cols), BF16),
        vm((ny, 2, nsp, 2 * cap, cols), BF16),
        vm((nslots, tokens), BF16),
        vm((tokens, nslots), BF16),
        vm((ny, 2, tokens, cols), BF16),
        vm((ny, 2, tokens, cols), BF16),
        vm((tokens, cols), F32),
        vm((nsp, 1, 128), F32),
        vm((tokens, tokens), F32),
        vm((tokens, tokens), F32),
        vm((8, tokens), F32),
        vm((nslots, units), F32),
        vm((nslots, units), F32),
        vm((nslots, units), F32),
        vm((nslots, units), BF16),
        vm((nslots, units), BF16),
        vm((nslots, units), BF16),
        vm((units, nslots), BF16),
        vm((units, nslots), BF16),
        vm((ny, nslots, cols), F32),
        vm((ny, nslots, cols), BF16),
        vm((ny, nslots, cols), BF16),
        vm((far, nslots, cols), BF16),
        vm((far, nslots, cols), BF16),
        vm((far, nslots, cols), BF16),
        vm((far, nslots, cols), BF16),
        vm((nsp, cap, cols), BF16),
        vm((nsp, cap, cols), BF16),
        vm((ntp, 1, 128), F32),
        vm((tokens, width), BF16),
        vm((units, width), BF16),
        vm((units, width), BF16),
        dma((2,)),
        vm((nx, dim // 2, 2 * dim), BF16),
        vm((nz, dim // 2, 2 * dim), BF16),
        vm((nsp, dim // 2, 2 * dim), BF16),
        vm((nsp, dim // 2, 2 * dim), BF16),
        dma((nsp,)),
        dma((nsp,)),
        dma((nsp,)),
        dma((nsp,)),
        dma((ny,)),
        dma((ny,)),
        dma((ny,)),
        dma((ny,)),
        dma((8 * far,)),
        dma((8 * far,)),
        dma((4 * ny,)),
        dma((4 * ny,)),
        dma((2 * ny,)),
        dma((2 * ny,)),
        dma((8 * far,)),
        dma((8 * far,)),
        dma((nsp,)),
        dma((nsp,)),
        dma((ny,)),
        dma((ny,)),
        dma((ny,)),
        dma((ny,)),
        dma((ntp,)),
        dma((ntp,)),
        dma((nx,)),
        dma((nx,)),
        dma((nz,)),
        dma((nz,)),
        dma((nsp,)),
        dma((nsp,)),
    ]
    outs = pl.pallas_call(
        functools.partial(body_kernel, nz, nx, ny),
        out_shape=(
            shape(up.shape, BF16),
            shape(down.shape, BF16),
            shape((width // nsp, dim), F32),
            shape(shape_t, BF16),
            shape(shape_t, BF16),
            shape(shape_t, BF16),
            shape(mixer_out.shape, BF16),
        ),
        in_specs=[hbm] * 16,
        out_specs=(hbm, hbm) + (vmem,) * 5,
        scratch_shapes=scratch,
        compiler_params=pltpu.CompilerParams(
            collective_id=0, has_side_effects=True, vmem_limit_bytes=62_000_000
        ),
    )(
        mixer_out,
        layer_grad,
        row_scale.reshape(1, tokens),
        norm_gain.reshape(ntp, cols),
        routes.T,
        route_weight.T,
        gate,
        up,
        down,
        query.T,
        key.T,
        value.T,
        retained.T,
        decay,
        entry,
        oproj,
    )
    outs = pl.pallas_call(
        deliver,
        out_shape=tuple(shape(o.shape, o.dtype) for o in outs),
        in_specs=[hbm] * 7,
        out_specs=(hbm,) * 7,
        scratch_shapes=[vm(o.shape, o.dtype) for o in outs] + [dma((7,)), dma((7,))],
    )(*outs)
    return (*outs[:3], outs[3].T, outs[4].T, outs[5].T, outs[6])


def specs():
    in_specs = (
        P("sp", "tp"),
        P("sp", "tp"),
        P("sp"),
        P(),
        P("sp", None),
        P("sp", None),
        P("sp", "tp", None),
        P("sp", "tp", None),
        P("sp", "tp", None),
        P("sp", "tp"),
        P("sp", "tp"),
        P("sp", "tp"),
        P("sp", "tp"),
        P("tp", "sp"),
        P("sp", "tp", None, None),
        P("tp", None),
    )
    out_specs = (
        P("sp", "tp", None),
        P("sp", "tp", None),
        P("sp", "tp"),
        P("sp", "tp"),
        P("sp", "tp"),
        P("sp", "tp"),
        P("sp", "tp"),
    )
    return in_specs, out_specs


def solution(mesh, nx=4):
    nsp, ntp = mesh.shape["sp"], mesh.shape["tp"]
    in_specs, out_specs = specs()
    return jax.shard_map(
        functools.partial(step, nsp // nx, nx, ntp // 2),
        mesh=mesh,
        in_specs=in_specs,
        out_specs=out_specs,
        check_vma=False,
    )
```

```python
import functools

import jax
import jax.numpy as jnp
from jax import lax
from jax.experimental import pallas as pl
from jax.experimental.pallas import tpu as pltpu
from jax.sharding import PartitionSpec as P

MESH = pl.DeviceIdType.MESH
F32, BF16 = jnp.float32, jnp.bfloat16
NEAR_TWO = False
NEAR_SHARE = 9
NN = (((1,), (0,)), ((), ()))
NT = (((1,), (1,)), ((), ()))
TN = (((0,), (0,)), ((), ()))


def dot(a, b, dims=NN):
    return lax.dot_general(a, b, dims, preferred_element_type=F32)


def exact(a, b, dims=NN):
    return lax.dot_general(
        a, b, dims, precision=lax.Precision.HIGHEST, preferred_element_type=F32
    )


def iota(shape, dim):
    return lax.broadcasted_iota(jnp.int32, shape, dim)


def packed(square):
    half = square.shape[0] // 2
    return jnp.concatenate([square[:half], square[half:]], axis=1)


def unpacked(rows):
    half = rows.shape[1] // 2
    return jnp.concatenate([rows[:, :half], rows[:, half:]], axis=0)


def body_kernel(
    nz,
    nx,
    ny,
    mix_h,
    lgr_h,
    rsc_h,
    gain_h,
    routes_h,
    rweight_h,
    gate_h,
    up_h,
    down_h,
    query_h,
    key_h,
    value_h,
    retained_h,
    decay_h,
    entry_h,
    oproj_h,
    gup_h,
    gdown_h,
    gproj,
    gquery,
    gkey,
    gvalue,
    sgrad,
    mix,
    lgr,
    rsc,
    gain,
    routes,
    rweight,
    query,
    key,
    value,
    retained,
    decay,
    entry,
    oproj,
    in_sem,
    wg,
    wu,
    wd,
    w_sem,
    disp,
    ag,
    slots,
    slots_t,
    bbuf,
    abuf,
    scales,
    scaleds,
    afull,
    cbuf,
    scores,
    decays,
    crow,
    pre_g,
    pre_u,
    pre_a,
    gg,
    ug,
    act,
    act_t,
    ug_t,
    part,
    xs,
    xr,
    scw,
    rcw,
    sccw,
    rccw,
    route,
    back,
    dots,
    sfull,
    gdown,
    gup,
    o_sem,
    ubuf,
    tbuf,
    gps,
    gpr,
    d_s,
    d_r,
    c_s,
    c_r,
    b_s,
    b_r,
    bp_s,
    bp_r,
    ag_s,
    ag_r,
    agp_s,
    agp_r,
    x_s,
    x_r,
    rs_s,
    rs_r,
    t_s,
    t_r,
    a_s,
    a_r,
    ap_s,
    ap_r,
    p_s,
    p_r,
    u_s,
    u_r,
    v_s,
    v_r,
    g_s,
    g_r,
):
    nsp, ntp, far = nz * nx, 2 * ny, ny // 2
    tokens, cols = mix.shape
    nslots = slots.shape[0]
    cap = nslots // nsp
    near_group = nsp * NEAR_SHARE // 32
    sizes = (near_group, near_group, nsp // 2 - near_group, nsp // 2 - near_group)
    starts = (0, near_group, 2 * near_group, nsp // 2 + near_group)
    scale = query.shape[0] ** -0.5
    me = lax.axis_index("sp")
    tp = lax.axis_index("tp")
    z, x = me // nx, me % nx
    y, c = tp // 2, tp % 2
    partner = (me, tp + 1 - 2 * c)
    ahead = [
        [(me, lax.rem(y + (hops if dirn == 0 else ny - hops), ny) * 2 + c) for hops in range(3)]
        for dirn in range(2)
    ]

    def wrap(v, n):
        return lax.rem(v + 2 * n, n)

    def offset(k):
        i, dx = k // nx, lax.rem(k, nx)
        dz = ((i + 1) // 2) * (2 * lax.rem(i, 2) - 1)
        return dz, dx

    def source(k):
        dz, dx = offset(k)
        return wrap(z + dz, nz) * nx + wrap(x + dx, nx)

    def target(k):
        dz, dx = offset(k)
        return wrap(z - dz, nz) * nx + wrap(x - dx, nx)

    def rcopy(src, dst, ssem, rsem, dev):
        return pltpu.make_async_remote_copy(
            src_ref=src,
            dst_ref=dst,
            send_sem=ssem,
            recv_sem=rsem,
            device_id=dev,
            device_id_type=MESH,
        )

    def loop(lo, hi, fn):
        def step(i, carry):
            fn(i)
            return carry

        lax.fori_loop(lo, hi, step, 0)

    barrier = pltpu.get_barrier_semaphore()

    def greet_sp(i):
        pl.semaphore_signal(
            barrier, inc=1, device_id=(lax.rem(me + i, nsp), tp), device_id_type=MESH
        )

    def greet_tp(i):
        pl.semaphore_signal(
            barrier, inc=1, device_id=(me, lax.rem(tp + i, ntp)), device_id_type=MESH
        )

    for i in range(1, nsp):
        greet_sp(i)
    for i in range(1, ntp):
        greet_tp(i)
    brought = [
        pltpu.make_async_copy(src, dst, in_sem.at[i])
        for i, (src, dst) in enumerate(
            (
                (mix_h, mix),
                (lgr_h, lgr),
                (rsc_h, rsc),
                (gain_h, gain),
                (routes_h, routes),
                (rweight_h, rweight),
                (decay_h, decay),
                (query_h, query),
                (key_h, key),
                (value_h, value),
                (retained_h, retained),
                (entry_h, entry),
                (oproj_h, oproj),
            )
        )
    ]
    for one in brought:
        one.start()
    loads = [
        pltpu.make_async_copy(src.at[0], dst, w_sem.at[i])
        for i, (src, dst) in enumerate(((gate_h, wg), (up_h, wu), (down_h, wd)))
    ]
    for load in loads:
        load.start()

    for one in brought[:7]:
        one.wait()
    rs_col = jnp.transpose(jnp.broadcast_to(rsc[...], (tokens, tokens)))[:, :1]
    gain_row = jnp.sum(
        jnp.where(iota(gain.shape, 0) == tp, gain[...].astype(F32), 0.0), axis=0, keepdims=True
    )
    scaled = mix[...].astype(F32) * rs_col
    scales[...] = jnp.broadcast_to(rs_col, (tokens, cols))
    scaleds[...] = scaled
    normed = (scaled * gain_row).astype(BF16)
    named = iota((nsp, tokens), 0)
    first = routes[0:1, :] == named
    second = routes[1:2, :] == named
    either = jnp.where(first | second, 1.0, 0.0)
    before = jnp.where(
        iota((tokens, tokens), 0) < iota((tokens, tokens), 1), 1.0, 0.0
    )
    rank = dot(either.astype(BF16), before.astype(BF16))
    spread = jnp.where(iota((nslots, nsp), 0) // cap == iota((nslots, nsp), 1), 1.0, 0.0)
    spread = spread.astype(BF16)
    place = lax.rem(iota((nslots, tokens), 0), cap).astype(F32)
    hit0 = dot(spread, jnp.where(first, rank, -1.0).astype(BF16)) == place
    hit1 = dot(spread, jnp.where(second, rank, -1.0).astype(BF16)) == place
    hits = jnp.where(hit0 | hit1, 1.0, 0.0)
    weight = jnp.where(hit0, rweight[0:1, :], 0.0) + jnp.where(hit1, rweight[1:2, :], 0.0)
    slot_weight = jnp.sum(weight, axis=1, keepdims=True)
    slots[...] = hits.astype(BF16)
    rows_n = dot(slots[...], normed).astype(BF16)
    rows_g = (dot(slots[...], lgr[...]) * slot_weight).astype(BF16)
    disp[:, 0:cap, :] = rows_n.reshape(nsp, cap, cols)
    disp[:, cap : 2 * cap, :] = rows_g.reshape(nsp, cap, cols)
    ag[y, c, 0] = disp[me]
    bbuf[y, c] = (scaled * rs_col).astype(BF16)

    incl = iota((tokens, tokens), 1) <= iota((tokens, tokens), 0)
    c_col = jnp.sum(
        jnp.where(incl, jnp.broadcast_to(decay[...], (tokens, tokens)), 0.0),
        axis=1,
        keepdims=True,
    )
    c_all = jnp.sum(decay[...], axis=1, keepdims=True)
    cbuf[me] = jnp.broadcast_to(c_all, cbuf.shape[1:])

    pl.semaphore_wait(barrier, nsp + ntp - 2)

    def send_rows(k):
        dev = target(k)
        rcopy(disp.at[dev], ag.at[y, c, k], d_s.at[k], d_r.at[k], (dev, tp)).start()

    def wait_rows(k):
        rcopy(disp.at[me], ag.at[y, c, k], d_s.at[k], d_r.at[k], (source(k), tp)).wait_recv()

    near = 2 * near_group
    loop(1, near, lambda k: send_rows(near - k))

    def peer(i):
        return (me, lax.rem(y + i, ny) * 2 + c)

    def send_b(i):
        rcopy(bbuf.at[y, c], bbuf.at[y, c], b_s.at[i], b_r.at[i], peer(i)).start()

    order = [far]
    for d in range(far - 1, 0, -1):
        order += [d, ny - d]
    early = [i for i in order if min(i, ny - i) <= 2]
    late = [i for i in order if i not in early]
    for i in early:
        send_b(i)

    for one in brought[7:]:
        one.wait()
    c_cols = jnp.broadcast_to(c_col, (tokens, tokens))
    c_rows = jnp.transpose(c_cols)
    gap = jnp.where(incl, c_cols - c_rows, 0.0)
    decays[...] = jnp.where(incl, jnp.exp(gap), 0.0)
    scores[...] = scale * dot(query[...], key[...], TN) * decays[...]
    crow[...] = c_rows[0:8, :]
    slots_t[...] = jnp.transpose(slots[...].astype(F32)).astype(BF16)
    pre_g[...] = jnp.zeros_like(pre_g)
    pre_u[...] = jnp.zeros_like(pre_u)
    pre_a[...] = jnp.zeros_like(pre_a)

    def left_rows(k):
        rcopy(disp.at[me], ag.at[y, c, k], d_s.at[k], d_r.at[k], partner).wait_send()

    loop(1, near, left_rows)
    loop(0, nsp - near, lambda k: send_rows(nsp - 1 - k))

    def rows_in(p):
        return slice(starts[2 * p] * cap, (starts[2 * p + 1] + sizes[2 * p + 1]) * cap)

    def group_rows(g):
        return slice(starts[g] * cap, (starts[g] + sizes[g]) * cap)

    def view(rows):
        return pl.ds(rows.start, rows.stop - rows.start)

    def yat(d):
        return wrap(y + d, ny)

    def part_of(yy, cc, g):
        return ag.at[yy, cc, pl.ds(starts[g], sizes[g])]

    def ring(dirn, d, g, hops=1):
        piece = part_of(yat(-d) if dirn == 0 else yat(d), c, g)
        i = (dirn * far + d + hops - 1) * 4 + g
        return rcopy(piece, piece, ag_s.at[i], ag_r.at[i], ahead[dirn][hops])

    def arrived(dirn, d, g):
        piece = part_of(yat(-d) if dirn == 0 else yat(d), c, g)
        i = (dirn * far + d - 1) * 4 + g
        return rcopy(piece, piece, ag_s.at[i], ag_r.at[i], partner)

    def pair(rel, g, cc):
        piece = part_of(yat(rel), cc, g)
        i = lax.rem(rel + ny, ny) * 4 + g
        return rcopy(piece, piece, agp_s.at[i], agp_r.at[i], partner)

    def sends(dirn, d, g):
        if d < far - 1:
            return (1, 2) if d == far - 2 and g >= 2 and g % 2 == dirn else (1,)
        return (1,) if d == far - 1 and g < 2 and g % 2 == dirn else ()

    def forward(dirn, d, g):
        for hops in sends(dirn, d, g):
            ring(dirn, d, g, hops).start()

    def span_of(yy):
        return pl.ds(pl.multiple_of(yy * 2 * cols, 2 * cols), 2 * cols)

    def rows_of(yy, lo, first_slot, count):
        return jnp.concatenate(
            [
                ag[yy, cc, first_slot : first_slot + count, lo : lo + cap, :].reshape(
                    count * cap, cols
                )
                for cc in range(2)
            ],
            axis=1,
        )

    def groups(p):
        return (2 * p, 2 * p + 1)

    def multiply(p, rel):
        for g in groups(p):
            pair(rel, g, 1 - c).wait_recv()
        yy = yat(rel)
        cut = span_of(yy)
        rows = rows_in(p)
        first_slot, count = starts[2 * p], 2 * sizes[2 * p]
        rows_n = rows_of(yy, 0, first_slot, count)
        rows_g = rows_of(yy, cap, first_slot, count)
        pre_g[rows, :] += dot(rows_n, wg[:, cut], NT)
        pre_u[rows, :] += dot(rows_n, wu[:, cut], NT)
        pre_a[rows, :] += dot(rows_g, wd[:, cut], NT)

    def own_out(p):
        for g in groups(p):
            forward(0, 0, g)
            forward(1, 0, g)
        for g in groups(p):
            pair(0, g, c).start()

    def gather_step(p, d):
        for g in groups(p):
            for dirn in range(2):
                arrived(dirn, d, g).wait_recv()
                forward(dirn, d, g)
                pair(-d if dirn == 0 else d, g, c).start()
        if d == 1:
            multiply(p, 0)
        else:
            multiply(p, 1 - d)
            multiply(p, d - 1)

    def gather_last(p):
        for g in groups(p):
            arrived(g % 2, far, g).wait_recv()
            pair(far, g, c).start()
        if far > 1:
            multiply(p, 1 - far)
            multiply(p, far - 1)
        else:
            multiply(p, 0)
        multiply(p, far)

    def pointwise(p):
        rows = rows_in(p)
        gate_pre, up_pre, act_grad = pre_g[rows, :], pre_u[rows, :], pre_a[rows, :]
        sig = 1.0 / (1.0 + jnp.exp(-gate_pre))
        silu = gate_pre * sig
        act[rows, :] = (silu * up_pre).astype(BF16)
        ug[rows, :] = (act_grad * silu).astype(BF16)
        gg[rows, :] = (act_grad * up_pre * sig * (1.0 + gate_pre * (1.0 - sig))).astype(BF16)

    def to_pair(p, i):
        rows = view(rows_in(p))
        return rcopy(
            xs.at[i, rows], xr.at[i, rows], x_s.at[2 * i + p], x_r.at[2 * i + p], partner
        )

    def partial(p, rel):
        rel = rel % ny
        rows = rows_in(p)
        cut = span_of(yat(rel))
        both = dot(gg[rows, :], wg[:, cut]) + dot(ug[rows, :], wu[:, cut])
        lo, hi = both[:, :cols], both[:, cols:]
        part[rel, rows, :] = jnp.where(c == 0, lo, hi)
        xs[rel, rows, :] = jnp.where(c == 0, hi, lo).astype(BF16)
        to_pair(p, rel).start()

    stage, land = (scw, sccw), (rcw, rccw)
    stopover = (NEAR_TWO, True)

    def joined(p, rel):
        to_pair(p, rel % ny).wait_recv()

    def summed(rel, g):
        rows = group_rows(g)
        return part[rel % ny, rows, :] + xr[rel % ny, rows, :].astype(F32)

    def hop(dirn, d, g):
        i = (dirn * far + d - 1) * 4 + g
        rows = view(group_rows(g))
        return rcopy(
            stage[dirn].at[d - 1, rows],
            land[dirn].at[d - 1, rows],
            rs_s.at[i],
            rs_r.at[i],
            ahead[dirn][(d if d <= 2 else d - 2) if stopover[g // 2] else 1],
        )

    def taken(dirn, d, g):
        hop(dirn, d, g).wait_recv()
        return land[dirn][d - 1, group_rows(g), :].astype(F32)

    def hops_for(d, g):
        return [g % 2] if d == far else [0, 1]

    def push(p, d):
        for g in groups(p):
            for dirn in hops_for(d, g):
                total = summed(d if dirn == 0 else -d, g)
                if d == 2 and far > 2:
                    for more in range(3, far + 1):
                        if dirn in hops_for(more, g):
                            total = total + taken(dirn, more, g)
                stage[dirn][d - 1, group_rows(g), :] = total.astype(BF16)
                hop(dirn, d, g).start()

    def pass_on(d, dirn, g):
        total = summed(d if dirn == 0 else -d, g)
        if d < far - 1 or (d == far - 1 and g % 2 == dirn):
            total = total + taken(dirn, d + 1, g)
        stage[dirn][d - 1, group_rows(g), :] = total.astype(BF16)
        hop(dirn, d, g).start()

    def send_back(k):
        rcopy(
            route.at[k], back.at[me], t_s.at[k], t_r.at[me], (source(k), tp)
        ).start()

    def ring_end(p):
        for g in reversed(groups(p)):
            total = summed(0, g)
            for d in (1, 2) if stopover[p] else (1,):
                for dirn in hops_for(d, g):
                    total = total + taken(dirn, d, g)
            route[starts[g] : starts[g] + sizes[g]] = (
                total.astype(BF16).reshape(sizes[g], cap, cols)
            )
            first, stop = max(starts[g], 1), starts[g] + sizes[g]
            loop(0, stop - first, lambda k, stop=stop: send_back(stop - 1 - k))
        if p == 0:
            back[me] = route[0]

    def reduce_stages(p):
        outer = [r for d in range(far, 2, -1) for r in {d, ny - d}]
        inner = [r for d in range(min(2, far), 0, -1) for r in {d, ny - d}] + [0]
        same = [(g % 2, g) for g in groups(p)]
        other = [(1 - g % 2, g) for g in groups(p)]

        def begin():
            pointwise(p)
            for rel in outer:
                partial(p, rel)

        def second():
            for rel in outer:
                joined(p, rel)
            if stopover[p]:
                for d in range(far, 2, -1):
                    push(p, d)
            else:
                for dirn, g in same:
                    pass_on(far, dirn, g)
                for dirn, g in other:
                    pass_on(far - 1, dirn, g)

        def third():
            for rel in inner:
                partial(p, rel)

        def fourth():
            for rel in inner:
                joined(p, rel)
            if stopover[p]:
                push(p, 1)
            else:
                for dirn, g in same:
                    pass_on(far - 1, dirn, g)

        def fifth():
            if stopover[p]:
                push(p, 2)
            else:
                for dirn, g in other + same:
                    pass_on(2, dirn, g)

        def sixth():
            if not stopover[p]:
                for dirn, g in other + same:
                    pass_on(1, dirn, g)

        return begin, second, third, fourth, fifth, sixth, lambda: ring_end(p)

    loop(1, near, wait_rows)
    own_out(0)

    def send_c(d):
        @pl.when(d != me)
        def _():
            rcopy(cbuf.at[me], cbuf.at[me], c_s.at[d], c_r.at[me], (d, tp)).start()

    loop(0, (z + 1) * nx, send_c)
    for load in loads:
        load.wait()
    first_sum, second_sum = reduce_stages(0), reduce_stages(1)
    gather_step(0, 1)
    loop(near, nsp, wait_rows)
    own_out(1)
    for d in range(2, far):
        gather_step(0, d)
        gather_step(1, d - 1)
    gather_last(0)
    first_sum[0]()
    gather_step(1, far - 1)
    first_sum[1]()
    first_sum[2]()
    gather_last(1)
    second_sum[0]()
    first_sum[3]()
    second_sum[1]()
    first_sum[4]()
    second_sum[2]()
    second_sum[3]()
    act_t[...] = jnp.transpose(act[...].astype(F32)).astype(BF16)
    ug_t[...] = jnp.transpose(ug[...].astype(F32)).astype(BF16)

    def weight_grads(i):
        cut = span_of(i)
        gdown[:, cut] = dot(act_t[...], rows_of(i, cap, 0, nsp)).astype(BF16)
        gup[:, cut] = dot(ug_t[...], rows_of(i, 0, 0, nsp)).astype(BF16)

    pending = list(range(ny))

    def some_grads(n):
        for _ in range(min(n, len(pending))):
            weight_grads(pending.pop(0))

    some_grads(1)
    second_sum[4]()
    first_sum[5]()
    some_grads(2)
    second_sum[6]()
    first_sum[6]()
    for i in late:
        send_b(i)

    some_grads(ny)
    outs = [
        pltpu.make_async_copy(gup, gup_h.at[0], o_sem.at[0]),
        pltpu.make_async_copy(gdown, gdown_h.at[0], o_sem.at[1]),
    ]
    for out in outs:
        out.start()

    def wait_back(i):
        e = lax.rem(me + i, nsp)
        rcopy(route.at[0], back.at[e], t_s.at[i], t_r.at[e], (e, tp)).wait_recv()

    def wait_back(i):
        e = lax.rem(me + i, nsp)
        rcopy(route.at[0], back.at[e], t_s.at[i], t_r.at[e], (e, tp)).wait_recv()

    def b_pair(i):
        yy = lax.rem(y + i, ny)
        return rcopy(bbuf.at[yy, c], bbuf.at[yy, c], bp_s.at[i], bp_r.at[i], partner)

    def b_pair_in(i):
        yy = lax.rem(y + i, ny)
        return rcopy(bbuf.at[yy, 1 - c], bbuf.at[yy, 1 - c], bp_s.at[i], bp_r.at[i], partner)

    def relay_b(i):
        yy = lax.rem(y + i, ny)
        rcopy(bbuf.at[yy, c], bbuf.at[yy, c], b_s.at[i], b_r.at[ny - i], peer(i)).wait_recv()
        b_pair(i).start()

    b_pair(0).start()
    for i in early:
        relay_b(i)

    loop(1, nsp, wait_back)
    hidden = dot(slots_t[...], back[...].reshape(nslots, cols)).astype(BF16).astype(F32)
    attend = gain_row * hidden
    rs_col, scaled = scales[...], scaleds[...]
    a32 = lgr[...].astype(F32) + rs_col * attend
    afull[...] = a32
    abuf[y, c] = a32.astype(BF16)
    def send_dot(i):
        rcopy(dots.at[y], dots.at[y], p_s.at[i], p_r.at[i], peer(i)).start()

    def wait_dot(i):
        yy = lax.rem(y + ny - i, ny)
        rcopy(dots.at[yy], dots.at[yy], p_s.at[i], p_r.at[i], peer(i)).wait_recv()

    def core_dot():
        return rcopy(dots.at[ny], dots.at[ny + 1], p_s.at[ny], p_r.at[ny], partner)

    def send_a(i):
        rcopy(abuf.at[y, c], abuf.at[y, c], a_s.at[i], a_r.at[i], peer(i)).start()

    def a_pair(i):
        yy = lax.rem(y + i, ny)
        return rcopy(abuf.at[yy, c], abuf.at[yy, c], ap_s.at[i], ap_r.at[i], partner)

    def a_pair_in(i):
        yy = lax.rem(y + i, ny)
        return rcopy(abuf.at[yy, 1 - c], abuf.at[yy, 1 - c], ap_s.at[i], ap_r.at[i], partner)

    def relay_a(i):
        yy = lax.rem(y + i, ny)
        rcopy(abuf.at[yy, c], abuf.at[yy, c], a_s.at[i], a_r.at[ny - i], peer(i)).wait_recv()
        a_pair(i).start()

    some = jnp.sum(scaled * attend, axis=1, keepdims=True)
    dots[y] = jnp.transpose(jnp.broadcast_to(some, (tokens, tokens)))[0:1, :]
    loop(1, ny, send_dot)
    for i in order:
        send_a(i)
    a_pair(0).start()
    for i in late:
        relay_b(i)
    for i in range(ny):
        b_pair_in(i).wait_recv()
    loop(1, ny, wait_dot)
    core_row = jnp.sum(dots[0:ny], axis=0)
    dots[ny] = core_row
    core_dot().start()
    core_dot().wait_recv()
    mean_row = (core_row + dots[ny + 1]) * (1.0 / (cols * ntp))
    mean_col = jnp.transpose(jnp.broadcast_to(mean_row, (tokens, tokens)))[:, :1]
    sgrad[...] = (afull[...] - (scaled * rs_col) * mean_col).astype(BF16)

    def stream(i, cc):
        yy = lax.rem(y + i, ny)
        cut = pl.ds(pl.multiple_of((yy * 2 + cc) * cols, cols), cols)
        sfull[:, cut] = (
            abuf[yy, cc].astype(F32) - bbuf[yy, cc].astype(F32) * mean_col
        ).astype(BF16)

    stream(0, c)
    for i in reversed(order):
        relay_a(i)
        stream(i, c)
    for i in [0] + order[::-1]:
        a_pair_in(i).wait_recv()
        stream(i, 1 - c)

    grad_out = dot(oproj[...], sfull[...], NT).astype(BF16)
    g32 = grad_out.astype(F32)
    rise = jnp.exp(crow[0:1, :])
    fall = jnp.exp(c_all - crow[0:1, :])
    update = exact(query[...].astype(F32) * rise, g32, NT)
    ubuf[x] = packed(update).astype(BF16)

    def send_u(i):
        xx = lax.rem(x + i, nx)
        rcopy(ubuf.at[x], ubuf.at[x], u_s.at[i], u_r.at[x], (z * nx + xx, tp)).start()

    def wait_u(i):
        xx = lax.rem(x + i, nx)
        rcopy(ubuf.at[xx], ubuf.at[xx], u_s.at[i], u_r.at[xx], (z * nx + xx, tp)).wait_recv()

    loop(1, nx, send_u)

    dim = retained.shape[0]
    proj = dot(retained[...], sfull[...])
    low = iota((dim // 2, 2 * dim), 1) < dim
    for j in range(nsp // 2):
        tile = proj[:, j * 2 * dim : (j + 1) * 2 * dim]
        turned = pltpu.roll(tile, dim, 1)
        gps[2 * j] = jnp.where(low, tile[: dim // 2], turned[dim // 2 :]).astype(BF16)
        gps[2 * j + 1] = jnp.where(low, turned[: dim // 2], tile[dim // 2 :]).astype(BF16)

    def send_g(k):
        dev = target(k)
        rcopy(gps.at[dev], gpr.at[k], g_s.at[k], g_r.at[k], (dev, tp)).start()

    loop(0, nsp - near, lambda i: send_g(nsp - 1 - i))

    def wait_c(i):
        m = z * nx + i

        @pl.when(m != me)
        def _():
            rcopy(cbuf.at[m], cbuf.at[m], c_s.at[m], c_r.at[m], (m, tp)).wait_recv()

    loop(0, nsp - z * nx, wait_c)
    loop(1, nx, wait_u)
    held = jnp.zeros((dim // 2, 2 * dim), F32)
    inside, after = held, jnp.zeros((1, 2 * dim), F32)
    for xx in range(nx - 1, -1, -1):
        drop = cbuf[z * nx + xx]
        inside = jnp.where(xx == x, held, inside)
        after = after + jnp.where(xx > x, drop, 0.0)
        held = ubuf[xx].astype(F32) + jnp.exp(drop) * held
    tbuf[z] = held.astype(BF16)

    def send_t(zz):
        rcopy(tbuf.at[z], tbuf.at[z], v_s.at[zz], v_r.at[z], (zz * nx + x, tp)).start()

    loop(0, z, send_t)
    loop(1, near, lambda k: send_g(near - k))
    gpr[0] = gps[me]

    q32, k32, v32 = query[...].astype(F32), key[...].astype(F32), value[...].astype(F32)
    press = scale * dot(grad_out, value[...], TN) * decays[...]
    gquery[...] = (
        exact(k32, press, NT) + scale * rise * exact(entry[0, 0], g32)
    ).astype(BF16)
    grad_key = exact(q32, press)
    grad_value = exact(g32, scores[...])

    for out in outs:
        out.wait()
    def sent_sp(k):
        rcopy(route.at[k], back.at[me], t_s.at[k], t_r.at[k], (source(k), tp)).wait_send()

    loop(near, nsp, left_rows)
    loop(1, nsp, sent_sp)

    def sent_c(d):
        @pl.when(d != me)
        def _():
            rcopy(cbuf.at[me], cbuf.at[me], c_s.at[d], c_r.at[me], (d, tp)).wait_send()

    loop(0, (z + 1) * nx, sent_c)

    def sent_u(i):
        rcopy(ubuf.at[x], ubuf.at[x], u_s.at[i], u_r.at[x], partner).wait_send()

    loop(1, nx, sent_u)

    def sent_t(zz):
        rcopy(tbuf.at[z], tbuf.at[z], v_s.at[zz], v_r.at[z], partner).wait_send()

    loop(0, z, sent_t)

    def sent_y(i):
        rcopy(bbuf.at[y, c], bbuf.at[y, c], b_s.at[i], b_r.at[i], peer(i)).wait_send()
        rcopy(abuf.at[y, c], abuf.at[y, c], a_s.at[i], a_r.at[i], peer(i)).wait_send()

    loop(1, ny, sent_y)

    def sent_pair(i):
        b_pair(i).wait_send()
        a_pair(i).wait_send()
        for g in range(4):
            pair(i, g, c).wait_send()
        for p in range(2):
            to_pair(p, i).wait_send()

    loop(0, ny, sent_pair)

    def sent_dot(i):
        rcopy(dots.at[y], dots.at[y], p_s.at[i], p_r.at[i], partner).wait_send()

    loop(1, ny + 1, sent_dot)
    for g in range(4):
        for dirn in range(2):
            for d in range(far):
                for hops in sends(dirn, d, g):
                    ring(dirn, d, g, hops).wait_send()
        for d in range(1, far + 1):
            for dirn in hops_for(d, g):
                hop(dirn, d, g).wait_send()

    def fold(i, carried):
        zz = nz - 1 - i
        rcopy(tbuf.at[zz], tbuf.at[zz], v_s.at[zz], v_r.at[zz], (zz * nx + x, tp)).wait_recv()
        drop = cbuf[zz * nx]
        for xx in range(1, nx):
            drop = drop + cbuf[zz * nx + xx]
        return tbuf[zz].astype(F32) + jnp.exp(drop) * carried

    beyond = lax.fori_loop(0, nz - 1 - z, fold, jnp.zeros((dim // 2, 2 * dim), F32))
    carried = unpacked(inside + jnp.exp(after) * beyond)
    gkey[...] = (grad_key + scale * fall * exact(carried, v32)).astype(BF16)
    gvalue[...] = (grad_value + scale * fall * exact(carried, k32, TN)).astype(BF16)

    def wait_g(k):
        rcopy(gps.at[me], gpr.at[k], g_s.at[k], g_r.at[k], (source(k), tp)).wait_recv()

    loop(1, nsp, wait_g)
    gproj[...] = jnp.transpose(unpacked(jnp.sum(gpr[...].astype(F32), axis=0)))

    def sent_g(k):
        rcopy(gps.at[me], gpr.at[k], g_s.at[k], g_r.at[k], (source(k), tp)).wait_send()

    loop(1, nsp, sent_g)

def deliver(*refs):
    sources, results, held, (taken, given) = refs[:7], refs[7:14], refs[14:21], refs[21:]
    moves = []
    for source, result, buffer in zip(sources, results, held):
        if len(source.shape) == 3:
            rows = source.shape[1] // 2
            for part in (pl.ds(0, rows), pl.ds(rows, rows)):
                moves.append((source.at[:, part], result.at[:, part], buffer.at[:, part]))
        else:
            moves.append((source, result, buffer))
    ins, copies = [], []
    for i, (source, result, buffer) in enumerate(moves):
        ins.append(pltpu.make_async_copy(source, buffer, taken.at[i]))
        copies.append(pltpu.make_async_copy(buffer, result, given.at[i]))
    for one in ins:
        one.start()
    for one, copy in zip(ins, copies):
        one.wait()
        copy.start()
    for copy in copies:
        copy.wait()


def step(nz, nx, ny, *args):
    (mixer_out, layer_grad, row_scale, norm_gain, routes, route_weight) = args[:6]
    (gate, up, down, query, key, value, retained, decay, entry, oproj) = args[6:]
    nsp, ntp, far = nz * nx, 2 * ny, ny // 2
    tokens, cols = mixer_out.shape
    fanout = routes.shape[1]
    cap = 2 * fanout * tokens // nsp
    nslots = nsp * cap
    units, width = gate.shape[1:]
    dim = query.shape[1]
    shape_t = (dim, tokens)
    vmem = pl.BlockSpec(memory_space=pltpu.VMEM)
    hbm = pl.BlockSpec(memory_space=pltpu.HBM)
    shape = jax.ShapeDtypeStruct
    dma = pltpu.SemaphoreType.DMA
    vm = pltpu.VMEM
    scratch = [
        vm((tokens, cols), BF16),
        vm((tokens, cols), BF16),
        vm((1, tokens), F32),
        vm((ntp, cols), BF16),
        vm((fanout, tokens), jnp.int32),
        vm((fanout, tokens), F32),
        vm((dim, tokens), BF16),
        vm((dim, tokens), BF16),
        vm((dim, tokens), BF16),
        vm((dim, tokens), BF16),
        vm((1, tokens), F32),
        vm(entry.shape, F32),
        vm(oproj.shape, BF16),
        dma((13,)),
        vm((units, width), BF16),
        vm((units, width), BF16),
        vm((units, width), BF16),
        dma((3,)),
        vm((nsp, 2 * cap, cols), BF16),
        vm((ny, 2, nsp, 2 * cap, cols), BF16),
        vm((nslots, tokens), BF16),
        vm((tokens, nslots), BF16),
        vm((ny, 2, tokens, cols), BF16),
        vm((ny, 2, tokens, cols), BF16),
        vm((tokens, cols), F32),
        vm((tokens, cols), F32),
        vm((tokens, cols), F32),
        vm((nsp, 1, 128), F32),
        vm((tokens, tokens), F32),
        vm((tokens, tokens), F32),
        vm((8, tokens), F32),
        vm((nslots, units), F32),
        vm((nslots, units), F32),
        vm((nslots, units), F32),
        vm((nslots, units), BF16),
        vm((nslots, units), BF16),
        vm((nslots, units), BF16),
        vm((units, nslots), BF16),
        vm((units, nslots), BF16),
        vm((ny, nslots, cols), F32),
        vm((ny, nslots, cols), BF16),
        vm((ny, nslots, cols), BF16),
        vm((far, nslots, cols), BF16),
        vm((far, nslots, cols), BF16),
        vm((far, nslots, cols), BF16),
        vm((far, nslots, cols), BF16),
        vm((nsp, cap, cols), BF16),
        vm((nsp, cap, cols), BF16),
        vm((ntp, 1, 128), F32),
        vm((tokens, width), BF16),
        vm((units, width), BF16),
        vm((units, width), BF16),
        dma((2,)),
        vm((nx, dim // 2, 2 * dim), BF16),
        vm((nz, dim // 2, 2 * dim), BF16),
        vm((nsp, dim // 2, 2 * dim), BF16),
        vm((nsp, dim // 2, 2 * dim), BF16),
        dma((nsp,)),
        dma((nsp,)),
        dma((nsp,)),
        dma((nsp,)),
        dma((ny,)),
        dma((ny,)),
        dma((ny,)),
        dma((ny,)),
        dma((8 * far,)),
        dma((8 * far,)),
        dma((4 * ny,)),
        dma((4 * ny,)),
        dma((2 * ny,)),
        dma((2 * ny,)),
        dma((8 * far,)),
        dma((8 * far,)),
        dma((nsp,)),
        dma((nsp,)),
        dma((ny,)),
        dma((ny,)),
        dma((ny,)),
        dma((ny,)),
        dma((ntp,)),
        dma((ntp,)),
        dma((nx,)),
        dma((nx,)),
        dma((nz,)),
        dma((nz,)),
        dma((nsp,)),
        dma((nsp,)),
    ]
    outs = pl.pallas_call(
        functools.partial(body_kernel, nz, nx, ny),
        out_shape=(
            shape(up.shape, BF16),
            shape(down.shape, BF16),
            shape((width // nsp, dim), F32),
            shape(shape_t, BF16),
            shape(shape_t, BF16),
            shape(shape_t, BF16),
            shape(mixer_out.shape, BF16),
        ),
        in_specs=[hbm] * 16,
        out_specs=(hbm, hbm) + (vmem,) * 5,
        scratch_shapes=scratch,
        compiler_params=pltpu.CompilerParams(
            collective_id=0, has_side_effects=True, vmem_limit_bytes=62_000_000
        ),
    )(
        mixer_out,
        layer_grad,
        row_scale.reshape(1, tokens),
        norm_gain.reshape(ntp, cols),
        routes.T,
        route_weight.T,
        gate,
        up,
        down,
        query.T,
        key.T,
        value.T,
        retained.T,
        decay,
        entry,
        oproj,
    )
    outs = pl.pallas_call(
        deliver,
        out_shape=tuple(shape(o.shape, o.dtype) for o in outs),
        in_specs=[hbm] * 7,
        out_specs=(hbm,) * 7,
        scratch_shapes=[vm(o.shape, o.dtype) for o in outs] + [dma((9,)), dma((9,))],
    )(*outs)
    return (*outs[:3], outs[3].T, outs[4].T, outs[5].T, outs[6])


def specs():
    in_specs = (
        P("sp", "tp"),
        P("sp", "tp"),
        P("sp"),
        P(),
        P("sp", None),
        P("sp", None),
        P("sp", "tp", None),
        P("sp", "tp", None),
        P("sp", "tp", None),
        P("sp", "tp"),
        P("sp", "tp"),
        P("sp", "tp"),
        P("sp", "tp"),
        P("tp", "sp"),
        P("sp", "tp", None, None),
        P("tp", None),
    )
    out_specs = (
        P("sp", "tp", None),
        P("sp", "tp", None),
        P("sp", "tp"),
        P("sp", "tp"),
        P("sp", "tp"),
        P("sp", "tp"),
        P("sp", "tp"),
    )
    return in_specs, out_specs


def solution(mesh, nx=4):
    nsp, ntp = mesh.shape["sp"], mesh.shape["tp"]
    in_specs, out_specs = specs()
    return jax.shard_map(
        functools.partial(step, nsp // nx, nx, ntp // 2),
        mesh=mesh,
        in_specs=in_specs,
        out_specs=out_specs,
        check_vma=False,
    )
```
